32 devices in a mesh: ep: 8 (over z, y), tp: 4 (over x, core).
Axes of the slice: x: 2, y: 2, z: 4, core: 2. Of those that a mesh axis runs over, the one named last changes fastest.
Arguments:
- tokens: bfloat16 [256, 2048], P('ep'), may hold values from -6 to 6
- kv_cache: bfloat16 [256, 1024, 512], P('ep', None, 'tp'), may hold values from -320 to 320
- lengths: int32 [256], P('ep'), may hold values from 1 to 1024, 131072 in all
- attn_gain: float32 [2048], replicated, may hold values from 0.1 to 1.9
- w_query: bfloat16 [2048, 1024], P(None, 'tp'), may hold values from -0.125 to 0.125
- w_key: bfloat16 [2048, 256], P(None, 'tp'), may hold values from -0.125 to 0.125
- w_value: bfloat16 [2048, 256], P(None, 'tp'), may hold values from -0.125 to 0.125
- lambdas: float32 [16], P('tp'), may hold values from 0.3 to 0.8
- head_gain: float32 [64], replicated, may hold values from 0.1 to 1.9
- w_out: bfloat16 [1024, 2048], replicated, may hold values from -0.1875 to 0.1875
- ffn_gain: float32 [2048], replicated, may hold values from 0.1 to 1.9
- w_shared_gate: bfloat16 [2048, 512], P(None, 'tp'), may hold values from -0.125 to 0.125
- w_shared_up: bfloat16 [2048, 512], P(None, 'tp'), may hold values from -0.125 to 0.125
- w_shared_down: bfloat16 [512, 2048], P('tp'), may hold values from -0.25 to 0.25
- routing: int32 [256, 4], replicated, may hold values from 0 to 31, all different within a row; in each aligned block of 32 rows (0 to 31, 32 to 63, ...) at most 8 rows name the same one
- route_weights: float32 [256, 4], P('ep'), may hold values from 0.1 to 1
- w_exp_gate: bfloat16 [32, 2048, 512], P(('ep', 'tp')), may hold values from -0.125 to 0.125
- w_exp_up: bfloat16 [32, 2048, 512], P(('ep', 'tp')), may hold values from -0.125 to 0.125
- w_exp_down: bfloat16 [32, 512, 2048], P(('ep', 'tp')), may hold values from -0.25 to 0.25
Outputs:
- mixed: bfloat16 [256, 2048], P('ep', 'tp')
The draws below stay inside these ranges and needn't reach their ends.
Inputs may be any that keep to these rules, and one draw needn't show every extreme that they name: `lengths`: A sequence's cache holds its past keys and values at positions below its length, and the new token follows them; some sequence uses all 1024 positions. `routing`: each row names 4 different experts. Within the rows of one group of 32 sequences (aligned blocks) no expert is named by more than 8 rows, and in some blocks an expert is named by exactly 8.
All inputs are finite; a program needn't handle non-finite values. No bound on the sum of `lengths` on one device may be relied on, other than what follows from the above.
Results may differ from the reference program's by a relative error of at most 0.015.
The reference program's roundings to bfloat16 on the way count: a program that leaves them out, or rounds other values in their place, can miss the bound.
Values may be sent and summed in bfloat16 or wider, within the bound.
No kernel may reach another device: no remote copies, remote signals or barrier semaphores. Data moves between devices by JAX's collectives and lax.ppermute only.
A program may use at most 128 MiB of HBM per device.

```python
import math
import jax
import jax.numpy as jnp
import numpy as np
from jax import lax

D = 2048
HEADS = 16
KV_HEADS = 4
QK_DIM = 32
V_DIM = 64
FF_S = 512
FF_E = 512
TOPK = 4
SEQ_DEV = 32
CACHE = 1024
BATCH = 256
EXPERTS = 32
CAP = 8
N_EP = 8
N_TP = 4


def draw_kv_cache(key, part):
    key_base = jax.random.fold_in(key, 0)
    full_shape = (BATCH, CACHE, KV_HEADS, 2, 2 * QK_DIM)
    base_draw = jax.random.normal(key_base, full_shape, jnp.float32)
    scales = jnp.array([1.75, 1.0], jnp.float32)
    entries = base_draw * scales[:, None]
    return entries.reshape(BATCH, CACHE, KV_HEADS * 4 * QK_DIM).astype(jnp.bfloat16)


def steps_of(key, dims, cuts, smallest, top_value):
    loudness = 1.0
    for dim, blocks in cuts:
        draws = jax.random.uniform(jax.random.fold_in(jax.random.fold_in(key, 6), dim), (blocks,), jnp.float32, smallest / len(cuts), top_value / len(cuts))
        loudness = loudness * jnp.repeat(jnp.exp(draws), dims[dim] // blocks).reshape((-1,) + (1,) * (len(dims) - 1 - dim))
    return loudness


def split_up(amount, total, reach, slope):
    loads = [(1 << 20) // math.isqrt(grade ** slope) + 1 for grade in range(2, amount + 1)]
    spare, counts = total - reach - (amount - 1), [1] * (amount - 1)
    while spare > 0:
        free = [i for i in range(amount - 1) if counts[i] < reach]
        mass, left = sum([loads[i] for i in free]), spare
        for i in free:
            extra = min(reach - counts[i], max(1, left * loads[i] // mass), spare)
            counts[i] = counts[i] + extra
            spare = spare - extra
    return np.array([reach] + counts)


def ragged_sizes(stream_key, number_of, total, most, lean):
    if number_of == 2:
        one = jax.random.randint(stream_key, (), max(1, total - most), min(most, total - 1) + 1)
        return jnp.stack([one, total - one])
    sizes = jnp.asarray(split_up(number_of, total, most, lean), jnp.int32)
    couples = (number_of - 1) // 2
    giver, taker = sizes[1:1 + 2 * couples:2], sizes[2:2 + 2 * couples:2]
    slack = jnp.minimum(giver - 1, most - taker)
    moved = jax.random.randint(jax.random.fold_in(stream_key, 1), (couples,), 0, 1 << 20) % (slack + 1)
    sizes = sizes.at[1:1 + 2 * couples:2].set(giver - moved).at[2:2 + 2 * couples:2].set(taker + moved)
    return sizes[jax.random.permutation(jax.random.fold_in(stream_key, 2), number_of)]


def shared_out(own_key, own, number, rows, number_of, top, bound, skew):
    sequence = jax.random.permutation(own_key, number_of)
    packed, common = load_shares(number_of, rows * top, bound, skew, True), load_shares(number_of, rows * top, bound, skew, False)
    places = jnp.arange(number_of)

    def named(sizes, rotation):
        used = int((sizes > 0).sum())
        fixed = max(1, used // 4)
        shifted = fixed + (places - fixed + rotation * (used - fixed)) % max(1, number_of - fixed)
        return jnp.zeros((number_of,), jnp.int32).at[sequence[jnp.where(places < fixed, places, shifted)]].set(jnp.asarray(sizes, jnp.int32))

    sizes = jnp.where(number % 4 == 0, named(packed, number // 4), named(common, number - number // 4 - 1))
    mixed = jax.random.permutation(jax.random.fold_in(own, 3), number_of)
    source_of, taker = mixed[0:number_of // 2 * 2:2], mixed[1:number_of // 2 * 2:2]
    room = jnp.minimum(sizes[source_of] - 1, bound - sizes[taker]) // 2
    room = jnp.where((source_of == sequence[0]) | (taker == sequence[0]) | (sizes[taker] == 0), 0, jnp.maximum(room, 0))
    shifted = jax.random.randint(jax.random.fold_in(own, 4), (number_of // 2,), 0, 1 << 20) % (room + 1)
    sizes = sizes.at[source_of].add(-shifted).at[taker].add(shifted)
    labels = jnp.searchsorted(jnp.cumsum(sizes), jnp.arange(rows * top), side="right").astype(jnp.int32)
    table = labels.reshape(top, rows).T
    table = table[jax.random.permutation(jax.random.fold_in(own, 1), rows)]
    rotation = jax.random.randint(jax.random.fold_in(own, 2), (rows, 1), 0, top)
    return jnp.take_along_axis(table, (jnp.arange(top)[None, :] + rotation) % top, axis=1)


def load_shares(count, total, reach, lean, full):
    loads = [(1 << 20) // math.isqrt(rank ** lean) + 1 for rank in range(1, count + 1)]
    largest = reach if full else min(reach, max(-(-total // count), total * loads[0] // sum(loads)))
    least = 1 if total - largest >= count - 1 else 0
    holding, rest = [largest] + [least] * (count - 1), total - largest - least * (count - 1)
    while rest > 0:
        movable = [i for i in range(1, count) if holding[i] < largest] or [i for i in range(1, count) if holding[i] < reach]
        whole, left = sum([loads[i] for i in movable]), rest
        for i in movable:
            extra = min(reach - holding[i], max(1, left * loads[i] // whole), rest)
            holding[i] = holding[i] + extra
            rest = rest - extra
    return np.array(holding)


def normal_values(stream_key, extent, width, bound, cuts=(), kind=jnp.bfloat16):
    drawn = width * jax.random.normal(stream_key, extent, jnp.float32)
    if cuts:
        drawn = drawn * steps_of(stream_key, extent, cuts, -0.22, 0.18)
    return jnp.clip(drawn, -bound, bound).astype(kind)


def setup_inputs(seed: int = 0) -> dict:
    streams_of = jax.random.split(jax.random.key(seed), 20)
    tokens = normal_values(streams_of[0], (BATCH, D), 1.0, 6.0, ((0, 8),))
    kv_cache = draw_kv_cache(jax.random.fold_in(streams_of[19], 71), 0)
    lengths = ragged_sizes(streams_of[2], BATCH, BATCH * CACHE // 2, CACHE, 2).astype(jnp.int32)
    attn_gain = jnp.clip(1.0 + 0.18 * jax.random.normal(streams_of[3], (D,), jnp.float32), 0.1, 1.9)
    w_query = normal_values(streams_of[4], (D, HEADS * 2 * QK_DIM), D ** -0.5, 0.125, ((1, 4),))
    w_key = normal_values(streams_of[5], (D, KV_HEADS * 2 * QK_DIM), D ** -0.5, 0.125, ((1, 4),))
    w_value = normal_values(streams_of[6], (D, KV_HEADS * V_DIM), D ** -0.5, 0.125, ((1, 4),))
    lambdas = jnp.clip(0.3 + 0.5 * jax.random.uniform(streams_of[7], (HEADS,), jnp.float32) ** steps_of(streams_of[7], (HEADS,), ((0, 4),), -0.2, 0.2), 0.3, 0.8)
    head_gain = jnp.clip(1.0 + 0.18 * jax.random.normal(streams_of[8], (V_DIM,), jnp.float32), 0.1, 1.9)
    w_out = normal_values(streams_of[9], (HEADS * V_DIM, D), (HEADS * V_DIM) ** -0.5, 0.1875)
    ffn_gain = jnp.clip(1.0 + 0.18 * jax.random.normal(streams_of[10], (D,), jnp.float32), 0.1, 1.9)
    w_shared_gate = normal_values(streams_of[11], (D, FF_S), D ** -0.5, 0.125, ((1, 4),))
    w_shared_up = normal_values(streams_of[12], (D, FF_S), D ** -0.5, 0.125, ((1, 4),))
    w_shared_down = normal_values(streams_of[13], (FF_S, D), FF_S ** -0.5, 0.25, ((0, 4),))
    routing_keys = jax.random.split(jax.random.fold_in(streams_of[14], 1), BATCH // SEQ_DEV)
    routing_turns = jax.random.permutation(jax.random.fold_in(streams_of[14], 3), BATCH // SEQ_DEV)
    routing = jax.vmap(lambda own, number: shared_out(jax.random.fold_in(streams_of[14], 2), own, number, SEQ_DEV, EXPERTS, TOPK, CAP, 2))(routing_keys, routing_turns).reshape((BATCH, TOPK))
    route_weights = jnp.clip(jnp.exp(math.log(1.0) - 2.3025851 * jax.random.uniform(streams_of[15], (BATCH, TOPK), jnp.float32) ** steps_of(streams_of[15], (BATCH, TOPK), ((0, 8),), -0.2, 0.2)), 0.1, 1.0)
    w_exp_gate = normal_values(streams_of[16], (EXPERTS, D, FF_E), D ** -0.5, 0.125, ((0, 32),))
    w_exp_up = normal_values(streams_of[17], (EXPERTS, D, FF_E), D ** -0.5, 0.125, ((0, 32),))
    w_exp_down = normal_values(streams_of[18], (EXPERTS, FF_E, D), FF_E ** -0.5, 0.25, ((0, 32),))
    return {"tokens": tokens, "kv_cache": kv_cache, "lengths": lengths, "attn_gain": attn_gain, "w_query": w_query, "w_key": w_key, "w_value": w_value, "lambdas": lambdas, "head_gain": head_gain, "w_out": w_out, "ffn_gain": ffn_gain, "w_shared_gate": w_shared_gate, "w_shared_up": w_shared_up, "w_shared_down": w_shared_down, "routing": routing, "route_weights": route_weights, "w_exp_gate": w_exp_gate, "w_exp_up": w_exp_up, "w_exp_down": w_exp_down}


epsilon = 1e-06
neg_fill = -1e+30

def norm_rows(values, gain_vec):
    widened = values.astype(jnp.float32)
    return widened * lax.rsqrt(lax.optimization_barrier(jnp.mean(widened * widened, axis=-1, keepdims=True)) + epsilon) * gain_vec

def group_sum(inner_act, weight):
    row_count = inner_act.shape[0]
    pieces = jnp.einsum('mtf,tfd->mtd', inner_act.reshape(row_count, N_TP, -1).astype(jnp.float32), weight.reshape(N_TP, -1, weight.shape[-1]).astype(jnp.float32))
    rounded = lax.optimization_barrier(pieces.astype(jnp.bfloat16))
    return lax.optimization_barrier(jnp.sum(rounded.astype(jnp.float32), axis=1))

def attend(block_q, block_k, block_v, block_cache, block_len, lambdas, head_gain):
    seq_total = block_q.shape[0]
    v_width = head_gain.shape[0]
    qk_width = v_width // 2
    kv_total = block_cache.shape[2] // (2 * v_width)
    group_size = lambdas.shape[0] // kv_total
    cache_len = block_cache.shape[1]
    queries = block_q.reshape(seq_total, kv_total, group_size, 2, qk_width).astype(jnp.float32)
    key_new = block_k.reshape(seq_total, kv_total, 2, qk_width).astype(jnp.float32)
    value_new = block_v.reshape(seq_total, kv_total, v_width).astype(jnp.float32)
    layout = block_cache.reshape(seq_total, cache_len, kv_total, 2 * v_width)
    keys_old = layout[..., :v_width].reshape(seq_total, cache_len, kv_total, 2, qk_width).astype(jnp.float32)
    values_old = layout[..., v_width:].astype(jnp.float32)
    scaling = qk_width ** (-0.5)
    scores_old = jnp.einsum('skgmd,sckmd->skgmc', queries, keys_old) * scaling
    scores_new = jnp.einsum('skgmd,skmd->skgm', queries, key_new) * scaling
    position = jnp.arange(cache_len, dtype=jnp.int32)
    valid_mask = (position[None, :] < block_len[:, None])[:, None, None, None, :]
    scores_old = jnp.where(valid_mask, scores_old, neg_fill)
    highest = jnp.maximum(lax.optimization_barrier(jnp.max(scores_old, axis=-1)), scores_new)
    expo_old = jnp.where(valid_mask, jnp.exp(scores_old - highest[..., None]), 0.0)
    expo_new = jnp.exp(scores_new - highest)
    totals = lax.optimization_barrier(jnp.sum(expo_old, axis=-1)) + expo_new
    lambda_grid = lambdas.reshape(kv_total, group_size)[None, :, :]
    weight_old = (expo_old[..., 0, :] / totals[..., 0, None] - lambda_grid[..., None] * expo_old[..., 1, :] / totals[..., 1, None]).astype(jnp.bfloat16)
    weight_new = (expo_new[..., 0] / totals[..., 0] - lambda_grid * expo_new[..., 1] / totals[..., 1]).astype(jnp.bfloat16)
    head_mix = jnp.einsum('skgc,sckv->skgv', weight_old.astype(jnp.float32), values_old)
    head_mix = head_mix + weight_new.astype(jnp.float32)[..., None] * value_new[:, :, None, :]
    return norm_rows(head_mix, head_gain).astype(jnp.bfloat16).reshape(seq_total, -1)

def reference(tokens, kv_cache, lengths, attn_gain, w_query, w_key, w_value, lambdas, head_gain, w_out, ffn_gain, w_shared_gate, w_shared_up, w_shared_down, routing, route_weights, w_exp_gate, w_exp_up, w_exp_down):
    normed = norm_rows(tokens, attn_gain).astype(jnp.bfloat16)
    queries = jnp.dot(normed, w_query, preferred_element_type=jnp.float32).astype(jnp.bfloat16)
    key_new = jnp.dot(normed, w_key, preferred_element_type=jnp.float32).astype(jnp.bfloat16)
    value_new = jnp.dot(normed, w_value, preferred_element_type=jnp.float32).astype(jnp.bfloat16)

    def attend_block(operands):
        return attend(operands[0], operands[1], operands[2], operands[3], operands[4], lambdas, head_gain)
    head_out = lax.map(attend_block, (queries.reshape(N_EP, SEQ_DEV, -1), key_new.reshape(N_EP, SEQ_DEV, -1), value_new.reshape(N_EP, SEQ_DEV, -1), kv_cache.reshape(N_EP, SEQ_DEV, CACHE, -1), lengths.reshape(N_EP, SEQ_DEV)))
    head_out = head_out.reshape(BATCH, HEADS * V_DIM)
    projected = group_sum(head_out, w_out)
    residual = (tokens.astype(jnp.float32) + projected).astype(jnp.bfloat16)
    ffn_in = norm_rows(residual, ffn_gain).astype(jnp.bfloat16)
    gate_vals = jnp.dot(ffn_in, w_shared_gate, preferred_element_type=jnp.float32)
    up_vals = jnp.dot(ffn_in, w_shared_up, preferred_element_type=jnp.float32)
    shared_act = (jax.nn.silu(gate_vals) * up_vals).astype(jnp.bfloat16)
    shared = jnp.dot(shared_act, w_shared_down, preferred_element_type=jnp.float32)
    grouped_ids = routing.reshape(N_EP, SEQ_DEV * TOPK)
    onehot = (grouped_ids[..., None] == jnp.arange(EXPERTS, dtype=jnp.int32)).astype(jnp.int32)
    slot_rank = lax.optimization_barrier(jnp.sum((jnp.cumsum(onehot, axis=1) - onehot) * onehot, axis=-1)).astype(jnp.int32)
    group_ids = jnp.broadcast_to(jnp.arange(N_EP, dtype=jnp.int32)[:, None], slot_rank.shape)
    rows_in = jnp.repeat(ffn_in.reshape(N_EP, SEQ_DEV, D), TOPK, axis=1)
    buffers = jnp.zeros((EXPERTS, N_EP, CAP, D), jnp.bfloat16).at[grouped_ids, group_ids, slot_rank].set(rows_in)

    def expert_apply(operands):
        row_block, gate_w, up_w, down_w = operands
        flat_rows = row_block.reshape(N_EP * CAP, D)
        gate_part = jnp.dot(flat_rows, gate_w, preferred_element_type=jnp.float32)
        up_part = jnp.dot(flat_rows, up_w, preferred_element_type=jnp.float32)
        inner_act = (jax.nn.silu(gate_part) * up_part).astype(jnp.bfloat16)
        result = jnp.dot(inner_act, down_w, preferred_element_type=jnp.float32).astype(jnp.bfloat16)
        return result.reshape(N_EP, CAP, D)
    expert_res = lax.map(expert_apply, (buffers, w_exp_gate, w_exp_up, w_exp_down))
    picked = expert_res[grouped_ids, group_ids, slot_rank].astype(jnp.float32)
    routed = lax.optimization_barrier(jnp.sum(route_weights.reshape(N_EP, SEQ_DEV, TOPK, 1) * picked.reshape(N_EP, SEQ_DEV, TOPK, D), axis=2))
    routed = routed.reshape(BATCH, D)
    return (residual.astype(jnp.float32) + shared + routed).astype(jnp.bfloat16)
```

```python
import functools

import jax
import jax.numpy as jnp
from jax import lax
from jax.experimental import pallas as pl
from jax.experimental.pallas import tpu as pltpu
from jax.sharding import PartitionSpec as P

epsilon = 1e-06
neg_fill = -1e30
f32 = jnp.float32
bf16 = jnp.bfloat16
VMEM = pl.BlockSpec(memory_space=pltpu.VMEM)
SMEM = pl.BlockSpec(memory_space=pltpu.SMEM)


def iota(shape, axis):
    return lax.broadcasted_iota(jnp.int32, shape, axis)


def dot(a, b):
    return jnp.dot(a, b, preferred_element_type=f32)


def inv_rms(values):
    return lax.rsqrt(jnp.mean(values * values, axis=-1, keepdims=True) + epsilon)


def slots_of(routing, experts, capacity):
    rows, top_count = routing.shape
    ids = iota((rows, experts), 1)
    hits = [routing[:, k : k + 1] == ids for k in range(top_count)]
    present = jnp.zeros((rows, experts), f32)
    for hit in hits:
        present = jnp.where(hit, 1.0, present)
    earlier = (iota((rows, rows), 1) < iota((rows, rows), 0)).astype(bf16)
    before = dot(earlier, present.astype(bf16))
    ranks = [jnp.sum(jnp.where(hit, before, 0.0), axis=1, keepdims=True) for hit in hits]
    return [
        routing[:, k : k + 1] * capacity + ranks[k].astype(jnp.int32) for k in range(top_count)
    ]


def attention_kernel(
    capacity,
    experts,
    lengths_ref,
    place_ref,
    lambdas_ref,
    tokens_ref,
    attn_gain_ref,
    w_query_ref,
    w_key_ref,
    w_value_ref,
    head_gain_ref,
    routing_ref,
    kv_ref,
    heads_ref,
    send_ref,
    q_scr,
    k_scr,
    v_scr,
    o_scr,
):
    step = pl.program_id(0)
    seqs, rows, lanes = q_scr.shape
    heads = rows // 2
    v_width = lanes // 2
    qk_width = v_width // 2
    block, cache_len, _ = kv_ref.shape
    scaling = qk_width ** (-0.5)

    @pl.when(step == 0)
    def _():
        tokens = tokens_ref[...].astype(f32)
        normed = (tokens * inv_rms(tokens) * attn_gain_ref[...]).astype(bf16)
        queries = dot(normed, w_query_ref[...]).astype(bf16).astype(f32)
        pad = jnp.zeros((seqs, v_width), f32)
        k_scr[...] = jnp.concatenate(
            [dot(normed, w_key_ref[...]).astype(bf16).astype(f32), pad], axis=1
        )
        v_scr[...] = jnp.concatenate(
            [pad, dot(normed, w_value_ref[...]).astype(bf16).astype(f32)], axis=1
        )
        lane = iota((seqs, lanes), 1)
        for h in range(heads):
            pair = queries[:, (h // 2) * lanes : (h // 2 + 1) * lanes]
            if h % 2:
                pair = pltpu.roll(pair, v_width, 1)
            for m in range(2):
                keep = (lane >= m * qk_width) & (lane < (m + 1) * qk_width)
                q_scr[:, m * heads + h, :] = jnp.where(keep, pair, 0.0)

    row = iota((rows, 1), 0)
    sign = jnp.where(row < heads, 1.0, 0.0)
    for h in range(heads):
        sign = jnp.where(row == heads + h, -lambdas_ref[h], sign)
    position = iota((rows, cache_len), 1)
    for b in range(block):
        s = step * block + b
        q = q_scr[s]
        cache = kv_ref[b]
        scores = (
            lax.dot_general(
                q.astype(bf16), cache, (((1,), (1,)), ((), ())), preferred_element_type=f32
            )
            * scaling
        )
        scores = jnp.where(position < lengths_ref[s], scores, neg_fill)
        fresh = jnp.sum(q * k_scr[pl.ds(s, 1), :], axis=1, keepdims=True) * scaling
        top = jnp.maximum(jnp.max(scores, axis=1, keepdims=True), fresh)
        expo = jnp.exp(scores - top)
        expo_new = jnp.exp(fresh - top)
        factor = sign / (jnp.sum(expo, axis=1, keepdims=True) + expo_new)
        part = expo * factor
        weights = (part + pltpu.roll(part, heads, 0)).astype(bf16)
        part_new = jnp.broadcast_to(expo_new * factor, (rows, lanes))
        weight_new = (part_new + pltpu.roll(part_new, heads, 0)).astype(bf16).astype(f32)
        o_scr[s] = dot(weights, cache) + weight_new * v_scr[pl.ds(s, 1), :]

    @pl.when(step == pl.num_programs(0) - 1)
    def _():
        lane = iota((seqs, lanes), 1)
        outs = []
        for h in range(heads):
            mix = jnp.where(lane >= v_width, o_scr[:, h, :], 0.0)
            mean = jnp.sum(mix * mix, axis=1, keepdims=True) * (1.0 / v_width)
            outs.append(mix * lax.rsqrt(mean + epsilon) * head_gain_ref[...])
        pairs = [
            jnp.where(lane < v_width, pltpu.roll(outs[2 * p], v_width, 1), outs[2 * p + 1])
            for p in range(heads // 2)
        ]
        head_out = jnp.concatenate(pairs, axis=1).astype(bf16)
        heads_ref[...] = head_out
        slots = slots_of(routing_ref[...], experts, capacity)
        ids = iota((seqs, experts * capacity), 1)
        picks = jnp.zeros((seqs, experts * capacity), f32)
        for slot in slots:
            picks = jnp.where(slot == ids, 1.0, picks)
        picks = picks.T.astype(bf16)
        width = head_out.shape[1]
        share = send_ref.shape[1] - width
        send_ref[:, :width] = dot(picks, head_out).astype(bf16)
        own = tokens_ref[:, pl.ds(pl.multiple_of(place_ref[0] * share, share), share)]
        send_ref[:, width:] = dot(picks, own).astype(bf16)


def expert_kernel(
    direct,
    arrived_ref,
    heads_ref,
    tokens_ref,
    w_out_ref,
    ffn_gain_ref,
    w_gate_ref,
    w_up_ref,
    w_down_ref,
    send_ref,
    ffn_ref,
    residual_ref,
    res_scr,
):
    groups, chunk, packed = arrived_ref.shape
    tp_count, seqs, width = heads_ref.shape
    capacity = chunk // tp_count
    rows = groups * capacity
    share = packed - width
    lefts = []
    tokens = []
    for j in range(tp_count):
        piece = arrived_ref[:, j * capacity : (j + 1) * capacity, :].astype(f32)
        piece = piece.reshape(rows, packed)
        lefts.append(jnp.concatenate([piece[:, :width].astype(bf16), heads_ref[j]], axis=0))
        own = tokens_ref[:, j * share : (j + 1) * share].astype(f32)
        tokens.append(jnp.concatenate([piece[:, width:], own], axis=0))
    square = jnp.zeros((rows + seqs, 1), f32)
    for n in range(tp_count):
        total = jnp.zeros((rows + seqs, share), f32)
        for j in range(tp_count):
            part = dot(
                lefts[j], w_out_ref[j * width : (j + 1) * width, n * share : (n + 1) * share]
            )
            total = total + part.astype(bf16).astype(f32)
        residual = (tokens[n] + total).astype(bf16)
        residual_ref[:, n * share : (n + 1) * share] = residual[rows:]
        residual = residual.astype(f32)
        res_scr[:, n * share : (n + 1) * share] = residual
        square = square + jnp.sum(residual * residual, axis=1, keepdims=True)
    scale = lax.rsqrt(square * (1.0 / res_scr.shape[1]) + epsilon)
    ffn_in = (res_scr[...] * scale * ffn_gain_ref[...]).astype(bf16)
    ffn_ref[...] = ffn_in[rows:]
    flat_rows = ffn_in[:rows]
    gate = dot(flat_rows, w_gate_ref[...])
    up = dot(flat_rows, w_up_ref[...])
    act = (gate / (1.0 + jnp.exp(-gate)) * up).astype(bf16)
    for j in range(tp_count):
        result = dot(act, w_down_ref[:, j * share : (j + 1) * share])
        if direct:
            for i in range(groups):
                send_ref[(i * tp_count + j) * capacity : (i * tp_count + j + 1) * capacity, :] = (
                    result[i * capacity : (i + 1) * capacity].astype(bf16)
                )
        else:
            send_ref[:, j * share : (j + 1) * share] = result.astype(bf16)


def shared_kernel(ffn_ref, w_gate_ref, w_up_ref, w_down_ref, part_ref):
    tp_count, _, share = part_ref.shape
    ffn_in = ffn_ref[...]
    gate = dot(ffn_in, w_gate_ref[...])
    up = dot(ffn_in, w_up_ref[...])
    act = (gate / (1.0 + jnp.exp(-gate)) * up).astype(bf16)
    for j in range(tp_count):
        part_ref[j] = dot(act, w_down_ref[:, j * share : (j + 1) * share]).astype(bf16)


def combine_kernel(
    capacity, experts, place_ref, residual_ref, part_ref, returned_ref, routing_ref, rates_ref, out_ref
):
    seqs, share = out_ref.shape
    slots = slots_of(routing_ref[...], experts, capacity)
    ids = iota((seqs, experts * capacity), 1)
    mixing = jnp.zeros((seqs, experts * capacity), f32)
    for k, slot in enumerate(slots):
        mixing = jnp.where(slot == ids, rates_ref[:, k : k + 1], mixing)
    high = mixing.astype(bf16)
    low = (mixing - high.astype(f32)).astype(bf16)
    returned = returned_ref[...]
    routed = dot(high, returned) + dot(low, returned)
    own = residual_ref[:, pl.ds(pl.multiple_of(place_ref[0] * share, share), share)].astype(f32)
    shared = jnp.zeros((seqs, share), f32)
    for j in range(part_ref.shape[0]):
        shared = shared + part_ref[j].astype(f32)
    out_ref[...] = (own + shared + routed).astype(bf16)


def params(mib, **more):
    return pltpu.CompilerParams(vmem_limit_bytes=mib << 20, **more)


def shards(
    tokens,
    kv_cache,
    lengths,
    attn_gain,
    w_query,
    w_key,
    w_value,
    lambdas,
    head_gain,
    w_out,
    ffn_gain,
    w_shared_gate,
    w_shared_up,
    w_shared_down,
    routing,
    route_weights,
    w_exp_gate,
    w_exp_up,
    w_exp_down,
):
    seqs, width = tokens.shape
    tp_count = lax.axis_size("tp")
    tp_index = lax.axis_index("tp")
    ep_count = lax.axis_size("ep")
    ep_index = lax.axis_index("ep")
    devices = ep_count * tp_count
    top_count = routing.shape[1]
    experts = w_exp_gate.shape[0] * devices
    capacity = max(2, 2 * seqs * top_count // experts)
    cache_len, lanes = kv_cache.shape[1:]
    v_width = head_gain.shape[0]
    heads = lambdas.shape[0]
    share = width // tp_count
    local = heads * v_width
    packed = local + share
    direct = capacity % 8 == 0
    own_routing = lax.dynamic_slice_in_dim(routing, ep_index * seqs, seqs, 0)
    place = tp_index.reshape(1).astype(jnp.int32)
    gain_row = jnp.concatenate([jnp.zeros((v_width,), f32), head_gain]).reshape(1, lanes)

    block = 4
    whole = lambda shape: pl.BlockSpec(shape, lambda i: (0,) * len(shape))
    head_out, send = pl.pallas_call(
        functools.partial(attention_kernel, capacity, experts),
        grid=(seqs // block,),
        in_specs=[
            SMEM,
            SMEM,
            SMEM,
            whole(tokens.shape),
            whole((1, width)),
            whole(w_query.shape),
            whole(w_key.shape),
            whole(w_value.shape),
            whole((1, lanes)),
            whole(own_routing.shape),
            pl.BlockSpec((block, cache_len, lanes), lambda i: (i, 0, 0)),
        ],
        out_specs=[whole((seqs, local)), whole((devices * capacity, packed))],
        out_shape=[
            jax.ShapeDtypeStruct((seqs, local), bf16),
            jax.ShapeDtypeStruct((devices * capacity, packed), bf16),
        ],
        scratch_shapes=[
            pltpu.VMEM((seqs, 2 * heads, lanes), f32),
            pltpu.VMEM((seqs, lanes), f32),
            pltpu.VMEM((seqs, lanes), f32),
            pltpu.VMEM((seqs, 2 * heads, lanes), f32),
        ],
        compiler_params=params(24),
        cost_estimate=pl.CostEstimate(
            flops=seqs * cache_len * lanes * 32, bytes_accessed=kv_cache.size * 2, transcendentals=0
        ),
        name="attention",
    )(
        lengths,
        place,
        lambdas,
        tokens,
        attn_gain.reshape(1, width),
        w_query,
        w_key,
        w_value,
        gain_row,
        own_routing,
        kv_cache,
    )

    arrived = lax.all_to_all(send, ("ep", "tp"), split_axis=0, concat_axis=0, tiled=True)
    all_heads = lax.all_gather(head_out, "tp", axis=0, tiled=False)

    rows = ep_count * capacity
    if direct:
        arrived = arrived.reshape(ep_count, tp_count * capacity, packed)
        sent_shape = (devices * capacity, share)
    else:
        arrived = arrived.reshape(ep_count, tp_count * capacity, packed)
        sent_shape = (rows, width)
    sent, ffn_own, residual = pl.pallas_call(
        functools.partial(expert_kernel, direct),
        in_specs=[VMEM] * 8,
        out_specs=[VMEM] * 3,
        out_shape=[
            jax.ShapeDtypeStruct(sent_shape, bf16),
            jax.ShapeDtypeStruct((seqs, width), bf16),
            jax.ShapeDtypeStruct((seqs, width), bf16),
        ],
        scratch_shapes=[pltpu.VMEM((rows + seqs, width), f32)],
        compiler_params=params(24),
        cost_estimate=pl.CostEstimate(
            flops=2 * 96 * 10 * (1 << 20), bytes_accessed=10 << 20, transcendentals=0
        ),
        name="experts",
    )(
        arrived,
        all_heads,
        tokens,
        w_out,
        ffn_gain.reshape(1, width),
        w_exp_gate.reshape(w_exp_gate.shape[1:]),
        w_exp_up.reshape(w_exp_up.shape[1:]),
        w_exp_down.reshape(w_exp_down.shape[1:]),
    )
    if not direct:
        sent = sent.reshape(ep_count, capacity, tp_count, share)
        sent = sent.transpose(0, 2, 1, 3).reshape(devices * capacity, share)
    returned = lax.all_to_all(sent, ("ep", "tp"), split_axis=0, concat_axis=0, tiled=True)

    part = pl.pallas_call(
        shared_kernel,
        in_specs=[VMEM] * 4,
        out_specs=VMEM,
        out_shape=jax.ShapeDtypeStruct((tp_count, seqs, share), bf16),
        compiler_params=params(16),
        cost_estimate=pl.CostEstimate(
            flops=2 * 32 * 3 * (1 << 18), bytes_accessed=3 << 19, transcendentals=0
        ),
        name="shared",
    )(ffn_own, w_shared_gate, w_shared_up, w_shared_down)
    parts = lax.all_to_all(part, "tp", split_axis=0, concat_axis=0, tiled=True)

    return pl.pallas_call(
        functools.partial(combine_kernel, capacity, experts),
        in_specs=[SMEM] + [VMEM] * 5,
        out_specs=VMEM,
        out_shape=jax.ShapeDtypeStruct((seqs, share), bf16),
        compiler_params=params(16),
        name="combine",
    )(place, residual, parts, returned, own_routing, route_weights)


def solution(mesh):
    return jax.shard_map(
        shards,
        mesh=mesh,
        in_specs=(
            P("ep", None),
            P("ep", None, "tp"),
            P("ep"),
            P(),
            P(None, "tp"),
            P(None, "tp"),
            P(None, "tp"),
            P("tp"),
            P(),
            P(),
            P(),
            P(None, "tp"),
            P(None, "tp"),
            P("tp", None),
            P(),
            P("ep", None),
            P(("ep", "tp"), None, None),
            P(("ep", "tp"), None, None),
            P(("ep", "tp"), None, None),
        ),
        out_specs=P("ep", "tp"),
        check_vma=False,
    )
```

```python
import functools

import jax
import jax.numpy as jnp
from jax import lax
from jax.experimental import pallas as pl
from jax.experimental.pallas import tpu as pltpu
from jax.sharding import PartitionSpec as P


epsilon = 1e-06
neg_fill = -1e30
f32 = jnp.float32
bf16 = jnp.bfloat16
VMEM = pl.BlockSpec(memory_space=pltpu.VMEM)
SMEM = pl.BlockSpec(memory_space=pltpu.SMEM)
HBM = pl.BlockSpec(memory_space=pltpu.HBM)


def iota(shape, axis):
    return lax.broadcasted_iota(jnp.int32, shape, axis)


def dot(a, b):
    return jnp.dot(a, b, preferred_element_type=f32)


def dot_nt(a, b):
    return lax.dot_general(a, b, (((1,), (1,)), ((), ())), preferred_element_type=f32)


def inv_rms(values):
    return lax.rsqrt(jnp.mean(values * values, axis=-1, keepdims=True) + epsilon)


def slots_of(routing, experts, capacity):
    rows, top_count = routing.shape
    ids = iota((rows, experts), 1)
    hits = [routing[:, k : k + 1] == ids for k in range(top_count)]
    present = jnp.zeros((rows, experts), f32)
    for hit in hits:
        present = jnp.where(hit, 1.0, present)
    earlier = (iota((rows, rows), 1) < iota((rows, rows), 0)).astype(bf16)
    before = dot(earlier, present.astype(bf16))
    ranks = [jnp.sum(jnp.where(hit, before, 0.0), axis=1, keepdims=True) for hit in hits]
    return [
        routing[:, k : k + 1] * capacity + ranks[k].astype(jnp.int32) for k in range(top_count)
    ]


def own_slots(routing_ref, slot_scr, seqs, experts, capacity):
    top_count, batch = routing_ref.shape
    pad = jnp.zeros((8 - top_count, batch), f32)
    slot_scr[...] = jnp.concatenate([routing_ref[...].astype(f32), pad], axis=0).T
    start = pl.multiple_of(lax.axis_index("ep") * seqs, seqs)
    own = slot_scr[pl.ds(start, seqs), :top_count].astype(jnp.int32)
    return slots_of(own, experts, capacity)


def attention_kernel(
    capacity,
    experts,
    block,
    tokens_hbm,
    attn_gain_hbm,
    w_query_hbm,
    w_key_hbm,
    w_value_hbm,
    head_gain_hbm,
    routing_hbm,
    lengths_hbm,
    lambdas_hbm,
    kv_hbm,
    heads_ref,
    send_ref,
    tokens_ref,
    attn_gain_ref,
    w_query_ref,
    w_key_ref,
    w_value_ref,
    head_gain_ref,
    routing_ref,
    lengths_ref,
    lambdas_ref,
    kv_ref,
    q_scr,
    k_scr,
    v_scr,
    o_scr,
    slot_scr,
    sems,
    kv_sems,
):
    seqs, rows, lanes = q_scr.shape
    heads = rows // 2
    v_width = lanes // 2
    qk_width = v_width // 2
    cache_len = kv_ref.shape[1]
    scaling = qk_width ** (-0.5)
    copies = [
        pltpu.make_async_copy(source, target, sems.at[i])
        for i, (source, target) in enumerate(
            [
                (tokens_hbm, tokens_ref),
                (attn_gain_hbm, attn_gain_ref),
                (w_query_hbm, w_query_ref),
                (w_key_hbm, w_key_ref),
                (w_value_hbm, w_value_ref),
                (lengths_hbm, lengths_ref),
                (lambdas_hbm, lambdas_ref),
                (head_gain_hbm, head_gain_ref),
                (routing_hbm, routing_ref),
            ]
        )
    ]
    for copy in copies:
        copy.start()
    steps = seqs // block
    streams = [
        pltpu.make_async_copy(
            kv_hbm.at[pl.ds(i * block, block)], kv_ref.at[pl.ds(i * block, block)], kv_sems.at[i]
        )
        for i in range(steps)
    ]
    for stream in streams[:2]:
        stream.start()
    for copy in copies[:5]:
        copy.wait()
    for stream in streams[2:]:
        stream.start()
    for copy in copies[5:]:
        copy.wait()

    tokens = tokens_ref[...].astype(f32)
    normed = (tokens * inv_rms(tokens) * attn_gain_ref[...]).astype(bf16)
    queries = dot(normed, w_query_ref[...]).astype(bf16).astype(f32)
    pad = jnp.zeros((seqs, v_width), f32)
    k_scr[...] = jnp.concatenate(
        [dot_nt(normed, w_key_ref[...]).astype(bf16).astype(f32), pad], axis=1
    )
    v_scr[...] = jnp.concatenate(
        [pad, dot_nt(normed, w_value_ref[...]).astype(bf16).astype(f32)], axis=1
    )
    lane = iota((seqs, lanes), 1)
    for h in range(heads):
        pair = queries[:, (h // 2) * lanes : (h // 2 + 1) * lanes]
        if h % 2:
            pair = pltpu.roll(pair, v_width, 1)
        for m in range(2):
            keep = (lane >= m * qk_width) & (lane < (m + 1) * qk_width)
            q_scr[:, m * heads + h, :] = jnp.where(keep, pair, 0.0)

    row = iota((rows, 1), 0)
    sign = jnp.where(row < heads, 1.0, 0.0)
    for h in range(heads):
        sign = jnp.where(row == heads + h, -lambdas_ref[h], sign)
    position = iota((rows, cache_len), 1)

    def scores_of(step):
        found = []
        for s in range(step * block, (step + 1) * block):
            found.append(dot_nt(q_scr[s].astype(bf16), kv_ref[s]))
        return found

    def finish(step, found):
        for b in range(block):
            s = step * block + b
            scores = jnp.where(position < lengths_ref[s], found[b] * scaling, neg_fill)
            fresh = jnp.sum(q_scr[s] * k_scr[s : s + 1, :], axis=1, keepdims=True) * scaling
            top = jnp.maximum(jnp.max(scores, axis=1, keepdims=True), fresh)
            expo = jnp.exp(scores - top)
            expo_new = jnp.exp(fresh - top)
            factor = sign / (jnp.sum(expo, axis=1, keepdims=True) + expo_new)
            part = expo * factor
            weights = (part + pltpu.roll(part, heads, 0)).astype(bf16)
            part_new = jnp.broadcast_to(expo_new * factor, (rows, lanes))
            weight_new = (part_new + pltpu.roll(part_new, heads, 0)).astype(bf16).astype(f32)
            o_scr[s] = dot(weights, kv_ref[s]) + weight_new * v_scr[s : s + 1, :]

    held = None
    for step in range(steps):
        streams[step].wait()
        found = scores_of(step)
        if held is not None:
            finish(step - 1, held)
        held = found
    finish(steps - 1, held)

    outs = []
    for h in range(heads):
        mix = jnp.where(lane >= v_width, o_scr[:, h, :], 0.0)
        mean = jnp.sum(mix * mix, axis=1, keepdims=True) * (1.0 / v_width)
        outs.append(mix * lax.rsqrt(mean + epsilon))
    gains = jnp.concatenate([head_gain_ref[...], head_gain_ref[...]], axis=1)
    pairs = [
        jnp.where(lane < v_width, pltpu.roll(outs[2 * p], v_width, 1), outs[2 * p + 1]) * gains
        for p in range(heads // 2)
    ]
    head_out = jnp.concatenate(pairs, axis=1).astype(bf16)
    heads_ref[...] = head_out
    slots = own_slots(routing_ref, slot_scr, seqs, experts, capacity)
    ids = iota((seqs, experts * capacity), 1)
    picks = jnp.zeros((seqs, experts * capacity), f32)
    for slot in slots:
        picks = jnp.where(slot == ids, 1.0, picks)
    picks = picks.T.astype(bf16)
    width = head_out.shape[1]
    share = send_ref.shape[1] - width
    send_ref[:, :width] = dot(picks, head_out).astype(bf16)
    start = pl.multiple_of(lax.axis_index("tp") * share, share)
    send_ref[:, width:] = dot(picks, tokens_ref[:, pl.ds(start, share)]).astype(bf16)


def silu(values):
    return values / (1.0 + jnp.exp(-values))


def partner(index, d, count):
    return index ^ d if count & (count - 1) == 0 else (index + d) % count


def own_kernel(
    capacity,
    experts,
    kept,
    heads_ref,
    w_out_hbm,
    tokens_hbm,
    gain_hbm,
    s_gate_hbm,
    s_up_hbm,
    s_down_hbm,
    routing_hbm,
    rates_hbm,
    *refs,
):
    tp_count, seqs, width = heads_ref.shape
    part_refs = refs[: tp_count - 1]
    base_ref, mix_ref, gain_ref, *kept_refs = refs[tp_count - 1 : tp_count + 2 + kept]
    refs = refs[tp_count + 2 + kept :]
    (
        tokens_ref,
        rest_ref,
        s_gate_ref,
        s_up_ref,
        s_down_ref,
        routing_ref,
        rates_ref,
        res_scr,
        slot_scr,
        sems,
    ) = refs
    share = base_ref.shape[1]
    blocks = column_blocks(w_out_hbm, rest_ref, kept_refs)
    early = [
        (tokens_hbm, tokens_ref),
        (gain_hbm, gain_ref),
        (routing_hbm, routing_ref),
        (rates_hbm, rates_ref),
        *blocks,
        (s_gate_hbm, s_gate_ref),
        (s_up_hbm, s_up_ref),
        (s_down_hbm, s_down_ref),
    ]
    copies = [
        pltpu.make_async_copy(source, target, sems.at[i])
        for i, (source, target) in enumerate(early)
    ]
    for copy in copies:
        copy.start()
    for copy in copies[:4]:
        copy.wait()
    slots = own_slots(routing_ref, slot_scr, seqs, experts, capacity)
    top_count = rates_ref.shape[0]
    rates = jnp.concatenate([rates_ref[...], jnp.zeros((8 - top_count, seqs), f32)], axis=0)
    rates = jnp.concatenate([rates, jnp.zeros((8, 128 - seqs), f32)], axis=1).T[:seqs]
    ids = iota((seqs, experts * capacity), 1)
    mixing = jnp.zeros((seqs, experts * capacity), f32)
    for k, slot in enumerate(slots):
        mixing = jnp.where(slot == ids, rates[:, k : k + 1], mixing)
    high = mixing.astype(bf16)
    mix_ref[:seqs] = high
    mix_ref[seqs:] = (mixing - high.astype(f32)).astype(bf16)

    square = jnp.zeros((seqs, 1), f32)
    for n in range(tp_count):
        copies[4 + n].wait()
        w_out_ref = blocks[n][1]
        cut = slice(n * share, (n + 1) * share)
        total = tokens_ref[:, cut].astype(f32)
        parts = jnp.zeros((seqs, share), f32)
        for j in range(tp_count):
            part = dot(heads_ref[j], w_out_ref[j * width : (j + 1) * width])
            parts = parts + part.astype(bf16).astype(f32)
        residual = (total + parts).astype(bf16).astype(f32)
        res_scr[:, cut] = residual
        square = square + jnp.sum(residual * residual, axis=1, keepdims=True)
    scale = lax.rsqrt(square * (1.0 / res_scr.shape[1]) + epsilon)
    ffn_in = (res_scr[...] * scale * gain_ref[...]).astype(bf16)
    for copy in copies[4 + tp_count :]:
        copy.wait()
    act = silu(dot(ffn_in, s_gate_ref[...])) * dot(ffn_in, s_up_ref[...])
    act = act.astype(bf16)
    for d in range(tp_count):
        start = pl.multiple_of(partner(lax.axis_index("tp"), d, tp_count) * share, share)
        part = dot(act, s_down_ref[:, pl.ds(start, share)])
        if d:
            part_refs[d - 1][...] = part.astype(bf16)
        else:
            base_ref[...] = res_scr[:, pl.ds(start, share)] + part


def column_blocks(w_out_hbm, rest_ref, kept_refs):
    share = rest_ref.shape[2]
    targets = [*kept_refs, *[rest_ref.at[i] for i in range(rest_ref.shape[0])]]
    return [
        (w_out_hbm.at[:, pl.ds(n * share, share)], target) for n, target in enumerate(targets)
    ]


def expert_kernel(
    direct,
    kept,
    arrived_ref,
    gain_ref,
    *refs,
):
    kept_refs = refs[:kept]
    (
        w_out_hbm,
        gate_hbm,
        up_hbm,
        down_hbm,
        send_hbm,
        send_ref,
        rest_ref,
        gate_ref,
        up_ref,
        down_ref,
        res_scr,
        sems,
    ) = refs[kept:]
    blocks = column_blocks(w_out_hbm, rest_ref, kept_refs)
    copies = [
        pltpu.make_async_copy(source, target, sems.at[i])
        for i, (source, target) in enumerate(
            [*blocks[kept:], (gate_hbm, gate_ref), (up_hbm, up_ref), (down_hbm, down_ref)]
        )
    ]
    for copy in copies:
        copy.start()
    groups, chunk, packed = arrived_ref.shape
    rows, model = res_scr.shape
    capacity = rows // groups
    tp_count = chunk // capacity
    share = model // tp_count
    width = packed - share
    lefts = []
    tokens = []
    for j in range(tp_count):
        piece = arrived_ref[:, j * capacity : (j + 1) * capacity, :].astype(f32)
        piece = piece.reshape(rows, packed)
        lefts.append(piece[:, :width].astype(bf16))
        tokens.append(piece[:, width:])
    square = jnp.zeros((rows, 1), f32)
    for n in range(tp_count):
        if n >= kept:
            copies[n - kept].wait()
        w_out_ref = blocks[n][1]
        cut = slice(n * share, (n + 1) * share)
        total = jnp.zeros((rows, share), f32)
        for j in range(tp_count):
            part = dot(lefts[j], w_out_ref[j * width : (j + 1) * width])
            total = total + part.astype(bf16).astype(f32)
        residual = (tokens[n] + total).astype(bf16).astype(f32)
        res_scr[:, cut] = residual
        square = square + jnp.sum(residual * residual, axis=1, keepdims=True)
    scale = lax.rsqrt(square * (1.0 / model) + epsilon)
    ffn_in = (res_scr[...] * scale * gain_ref[...]).astype(bf16)
    copies[-3].wait()
    gate = dot(ffn_in, gate_ref[...])
    copies[-2].wait()
    act = (silu(gate) * dot(ffn_in, up_ref[...])).astype(bf16)
    copies[-1].wait()
    for n in range(tp_count):
        result = dot(act, down_ref[:, n * share : (n + 1) * share])
        if direct:
            for i in range(groups):
                first = (i * tp_count + n) * capacity
                send_ref[first : first + capacity, :] = result[
                    i * capacity : (i + 1) * capacity
                ].astype(bf16)
        else:
            send_ref[:, n * share : (n + 1) * share] = result.astype(bf16)
    back = pltpu.make_async_copy(send_ref, send_hbm, sems.at[0])
    back.start()
    back.wait()


def combine_kernel(base_ref, mix_ref, returned_ref, *refs):
    *part_refs, out_ref = refs
    seqs = out_ref.shape[0]
    returned = returned_ref[...]
    routed = dot(mix_ref[...], returned)
    shared = base_ref[...]
    for part_ref in part_refs:
        shared = shared + part_ref[...].astype(f32)
    out_ref[...] = (shared + routed[:seqs] + routed[seqs:]).astype(bf16)


def params(mib, **more):
    return pltpu.CompilerParams(vmem_limit_bytes=mib << 20, **more)


def shards(
    tokens,
    kv_cache,
    lengths,
    attn_gain,
    w_query,
    w_key,
    w_value,
    lambdas,
    head_gain,
    w_out,
    ffn_gain,
    w_shared_gate,
    w_shared_up,
    w_shared_down,
    routing,
    route_weights,
    w_exp_gate,
    w_exp_up,
    w_exp_down,
):
    seqs, width = tokens.shape
    tp_count = lax.axis_size("tp")
    ep_count = lax.axis_size("ep")
    devices = ep_count * tp_count
    top_count = routing.shape[1]
    experts = w_exp_gate.shape[0] * devices
    capacity = max(2, 2 * seqs * top_count // experts)
    cache_len, lanes = kv_cache.shape[1:]
    v_width = head_gain.shape[0]
    heads = lambdas.shape[0]
    share = width // tp_count
    local = heads * v_width
    packed = local + share
    direct = capacity % 8 == 0
    block = 4
    head_out, send = pl.pallas_call(
        functools.partial(attention_kernel, capacity, experts, block),
        in_specs=[HBM] * 10,
        out_specs=[VMEM] * 2,
        out_shape=[
            pltpu.VMEM((seqs, local), bf16),
            jax.ShapeDtypeStruct((devices * capacity, packed), bf16),
        ],
        scratch_shapes=[
            pltpu.VMEM(tokens.shape, bf16),
            pltpu.VMEM((1, width), f32),
            pltpu.VMEM(w_query.shape, bf16),
            pltpu.VMEM(w_key.shape[::-1], bf16),
            pltpu.VMEM(w_value.shape[::-1], bf16),
            pltpu.VMEM((1, v_width), f32),
            pltpu.VMEM(routing.shape[::-1], jnp.int32),
            pltpu.SMEM(lengths.shape, jnp.int32),
            pltpu.SMEM(lambdas.shape, f32),
            pltpu.VMEM(kv_cache.shape, bf16),
            pltpu.VMEM((seqs, 2 * heads, lanes), f32),
            pltpu.VMEM((seqs, lanes), f32),
            pltpu.VMEM((seqs, lanes), f32),
            pltpu.VMEM((seqs, 2 * heads, lanes), f32),
            pltpu.VMEM((routing.shape[0], 8), f32),
            pltpu.SemaphoreType.DMA((9,)),
            pltpu.SemaphoreType.DMA((seqs // block,)),
        ],
        compiler_params=pltpu.CompilerParams(vmem_limit_bytes=67_043_328 - 2 * seqs * local),
        cost_estimate=pl.CostEstimate(
            flops=seqs * cache_len * lanes * 32, bytes_accessed=kv_cache.size * 2, transcendentals=0
        ),
        name="attention",
    )(
        tokens,
        attn_gain.reshape(1, width),
        w_query,
        w_key.T,
        w_value.T,
        head_gain.reshape(1, v_width),
        routing.T,
        lengths,
        lambdas,
        kv_cache,
    )

    arrived = lax.all_to_all(send, ("ep", "tp"), split_axis=0, concat_axis=0, tiled=True)
    arrived = arrived.reshape(ep_count, tp_count * capacity, packed)
    all_heads = lax.all_gather(head_out, "tp", axis=0, tiled=False)

    exp_gate = w_exp_gate.reshape(w_exp_gate.shape[1:])
    exp_up = w_exp_up.reshape(w_exp_up.shape[1:])
    exp_down = w_exp_down.reshape(w_exp_down.shape[1:])
    rows = ep_count * capacity
    slot_count = experts * capacity
    kept = 1
    w_out_block = (w_out.shape[0], share)
    rest = pltpu.VMEM((tp_count - kept, *w_out_block), bf16)
    results = pl.pallas_call(
        functools.partial(own_kernel, capacity, experts, kept),
        in_specs=[VMEM] + [HBM] * 8,
        out_specs=[VMEM] * (tp_count + 2 + kept),
        out_shape=[pltpu.VMEM((seqs, share), bf16)] * (tp_count - 1)
        + [
            pltpu.VMEM((seqs, share), f32),
            pltpu.VMEM((2 * seqs, slot_count), bf16),
            pltpu.VMEM((1, width), f32),
        ]
        + [pltpu.VMEM(w_out_block, bf16)] * kept,
        scratch_shapes=[
            pltpu.VMEM(tokens.shape, bf16),
            rest,
            pltpu.VMEM(w_shared_gate.shape, bf16),
            pltpu.VMEM(w_shared_up.shape, bf16),
            pltpu.VMEM(w_shared_down.shape, bf16),
            pltpu.VMEM(routing.shape[::-1], jnp.int32),
            pltpu.VMEM(route_weights.shape[::-1], f32),
            pltpu.VMEM((seqs, width), f32),
            pltpu.VMEM((routing.shape[0], 8), f32),
            pltpu.SemaphoreType.DMA((7 + tp_count,)),
        ],
        compiler_params=pltpu.CompilerParams(vmem_limit_bytes=63_900_000),
        cost_estimate=pl.CostEstimate(
            flops=2 * seqs * w_out.size, bytes_accessed=12 << 20, transcendentals=0
        ),
        name="own",
    )(
        all_heads,
        w_out,
        tokens,
        ffn_gain.reshape(1, width),
        w_shared_gate,
        w_shared_up,
        w_shared_down,
        routing.T,
        route_weights.T,
    )

    part, (base, mix, gain), kept_blocks = (
        results[: tp_count - 1],
        results[tp_count - 1 : tp_count + 2],
        results[tp_count + 2 :],
    )
    arrived, gain, *kept_blocks = [
        pltpu.with_memory_space_constraint(value, pltpu.VMEM)
        for value in (arrived, gain, *kept_blocks)
    ]
    sent_shape = (devices * capacity, share) if direct else (rows, width)
    sent = pl.pallas_call(
        functools.partial(expert_kernel, direct, kept),
        in_specs=[VMEM] * (2 + kept) + [HBM] * 4,
        out_specs=HBM,
        out_shape=jax.ShapeDtypeStruct(sent_shape, bf16),
        scratch_shapes=[
            pltpu.VMEM(sent_shape, bf16),
            rest,
            pltpu.VMEM(exp_gate.shape, bf16),
            pltpu.VMEM(exp_up.shape, bf16),
            pltpu.VMEM(exp_down.shape, bf16),
            pltpu.VMEM((rows, width), f32),
            pltpu.SemaphoreType.DMA((3 + tp_count - kept,)),
        ],
        compiler_params=pltpu.CompilerParams(vmem_limit_bytes=60 * 1024 * 1024),
        cost_estimate=pl.CostEstimate(
            flops=2 * rows * 5 * w_out.size // 2, bytes_accessed=1 << 20, transcendentals=0
        ),
        name="experts",
    )(arrived, gain, *kept_blocks, w_out, exp_gate, exp_up, exp_down)
    if not direct:
        sent = sent.reshape(ep_count, capacity, tp_count, share)
        sent = sent.transpose(0, 2, 1, 3).reshape(devices * capacity, share)
    returned = lax.all_to_all(sent, ("ep", "tp"), split_axis=0, concat_axis=0, tiled=True)
    parts = [
        lax.ppermute(piece, "tp", [(i, partner(i, d, tp_count)) for i in range(tp_count)])
        for d, piece in enumerate(part, 1)
    ]

    return pl.pallas_call(
        combine_kernel,
        in_specs=[VMEM] * (tp_count + 2),
        out_specs=VMEM,
        out_shape=jax.ShapeDtypeStruct((seqs, share), bf16),
        compiler_params=params(16),
        name="combine",
    )(base, mix, returned, *parts)


def solution(mesh):
    return jax.shard_map(
        shards,
        mesh=mesh,
        in_specs=(
            P("ep", None),
            P("ep", None, "tp"),
            P("ep"),
            P(),
            P(None, "tp"),
            P(None, "tp"),
            P(None, "tp"),
            P("tp"),
            P(),
            P(),
            P(),
            P(None, "tp"),
            P(None, "tp"),
            P("tp", None),
            P(),
            P("ep", None),
            P(("ep", "tp"), None, None),
            P(("ep", "tp"), None, None),
            P(("ep", "tp"), None, None),
        ),
        out_specs=P("ep", "tp"),
        check_vma=False,
    )
```

```python
import functools

import jax
import jax.numpy as jnp
from jax import lax
from jax.experimental import pallas as pl
from jax.experimental.pallas import tpu as pltpu
from jax.sharding import PartitionSpec as P


epsilon = 1e-06
neg_fill = -1e30
f32 = jnp.float32
bf16 = jnp.bfloat16
VMEM = pl.BlockSpec(memory_space=pltpu.VMEM)
SMEM = pl.BlockSpec(memory_space=pltpu.SMEM)
HBM = pl.BlockSpec(memory_space=pltpu.HBM)


def iota(shape, axis):
    return lax.broadcasted_iota(jnp.int32, shape, axis)


def dot(a, b):
    return jnp.dot(a, b, preferred_element_type=f32)


def dot_nt(a, b):
    return lax.dot_general(a, b, (((1,), (1,)), ((), ())), preferred_element_type=f32)


def inv_rms(values):
    return lax.rsqrt(jnp.mean(values * values, axis=-1, keepdims=True) + epsilon)


def slots_of(routing, experts, capacity):
    rows, top_count = routing.shape
    ids = iota((rows, experts), 1)
    hits = [routing[:, k : k + 1] == ids for k in range(top_count)]
    present = jnp.zeros((rows, experts), f32)
    for hit in hits:
        present = jnp.where(hit, 1.0, present)
    earlier = (iota((rows, rows), 1) < iota((rows, rows), 0)).astype(bf16)
    before = dot(earlier, present.astype(bf16))
    ranks = [jnp.sum(jnp.where(hit, before, 0.0), axis=1, keepdims=True) for hit in hits]
    return [
        routing[:, k : k + 1] * capacity + ranks[k].astype(jnp.int32) for k in range(top_count)
    ]


def own_slots(routing_ref, slot_scr, seqs, experts, capacity):
    top_count, batch = routing_ref.shape
    pad = jnp.zeros((8 - top_count, batch), f32)
    slot_scr[...] = jnp.concatenate([routing_ref[...].astype(f32), pad], axis=0).T
    start = pl.multiple_of(lax.axis_index("ep") * seqs, seqs)
    own = slot_scr[pl.ds(start, seqs), :top_count].astype(jnp.int32)
    return slots_of(own, experts, capacity)


def attention_kernel(
    capacity,
    experts,
    block,
    tokens_hbm,
    attn_gain_hbm,
    w_query_hbm,
    w_key_hbm,
    w_value_hbm,
    head_gain_hbm,
    routing_hbm,
    lengths_hbm,
    lambdas_hbm,
    kv_hbm,
    heads_ref,
    send_hbm,
    tokens_ref,
    attn_gain_ref,
    w_query_ref,
    w_key_ref,
    w_value_ref,
    head_gain_ref,
    routing_ref,
    lengths_ref,
    lambdas_ref,
    kv_ref,
    q_scr,
    k_scr,
    v_scr,
    o_scr,
    slot_scr,
    back_scr,
    mix_scr,
    sems,
    kv_sems,
    back_sems,
):
    seqs, rows, lanes = q_scr.shape
    heads = rows // 2
    v_width = lanes // 2
    qk_width = v_width // 2
    cache_len = kv_ref.shape[1]
    width = mix_scr.shape[1]
    share = back_scr.shape[1]
    scaling = qk_width ** (-0.5)
    copies = [
        pltpu.make_async_copy(source, target, sems.at[i])
        for i, (source, target) in enumerate(
            [
                (tokens_hbm, tokens_ref),
                (attn_gain_hbm, attn_gain_ref),
                (routing_hbm, routing_ref),
                (w_query_hbm, w_query_ref),
                (w_key_hbm, w_key_ref),
                (w_value_hbm, w_value_ref),
                (lengths_hbm, lengths_ref),
                (lambdas_hbm, lambdas_ref),
                (head_gain_hbm, head_gain_ref),
            ]
        )
    ]
    for copy in copies:
        copy.start()
    steps = seqs // block
    streams = [
        pltpu.make_async_copy(
            kv_hbm.at[pl.ds(i * block, block)], kv_ref.at[pl.ds(i * block, block)], kv_sems.at[i]
        )
        for i in range(steps)
    ]
    streams[0].start()
    for copy in copies[:3]:
        copy.wait()
    for stream in streams[1:]:
        stream.start()

    slots = own_slots(routing_ref, slot_scr, seqs, experts, capacity)
    ids = iota((seqs, experts * capacity), 1)
    picks = jnp.zeros((seqs, experts * capacity), f32)
    for slot in slots:
        picks = jnp.where(slot == ids, 1.0, picks)
    picks = picks.T.astype(bf16)
    start = pl.multiple_of(lax.axis_index("tp") * share, share)
    back_scr[...] = dot(picks, tokens_ref[:, pl.ds(start, share)]).astype(bf16)
    backs = [
        pltpu.make_async_copy(back_scr, send_hbm.at[:, pl.ds(width, share)], back_sems.at[0]),
        pltpu.make_async_copy(mix_scr, send_hbm.at[:, pl.ds(0, width)], back_sems.at[1]),
    ]
    backs[0].start()
    tokens = tokens_ref[...].astype(f32)
    normed = (tokens * inv_rms(tokens) * attn_gain_ref[...]).astype(bf16)

    for copy in copies[3:]:
        copy.wait()
    queries = dot(normed, w_query_ref[...]).astype(bf16).astype(f32)
    key_new = dot_nt(normed, w_key_ref[...]).astype(bf16).astype(f32)
    value_new = dot_nt(normed, w_value_ref[...]).astype(bf16).astype(f32)
    k_scr[...] = jnp.concatenate([key_new, key_new], axis=1)
    v_scr[...] = jnp.concatenate([value_new, value_new], axis=1)
    lane = iota((seqs, lanes), 1)
    upper = lane >= v_width
    own_keys = upper == (iota((seqs, lanes), 0) % 2 == 1)
    for h in range(heads):
        pair = queries[:, (h // 2) * lanes : (h // 2 + 1) * lanes]
        pair = jnp.where(upper == (h % 2 == 1), pair, pltpu.roll(pair, v_width, 1))
        for m in range(2):
            inner = lane % v_width
            keep = own_keys & (inner >= m * qk_width) & (inner < (m + 1) * qk_width)
            q_scr[:, m * heads + h, :] = jnp.where(keep, pair, 0.0)

    row = iota((2 * rows, 1), 0) % rows
    sign = jnp.where(row < heads, 1.0, 0.0)
    for h in range(heads):
        sign = jnp.where(row == heads + h, -lambdas_ref[h], sign)
    position = iota((2 * rows, cache_len), 1)
    second = iota((2 * rows, 1), 0) >= rows

    def scores_of(step):
        found = []
        for b in range(0, block, 2):
            s = step * block + b
            even, odd = kv_ref[s], kv_ref[s + 1]
            query = q_scr[s : s + 2].reshape(2 * rows, lanes).astype(bf16)
            keys = jnp.concatenate([even[:, :v_width], odd[:, :v_width]], axis=1)
            values = jnp.concatenate([odd[:, v_width:], even[:, v_width:]], axis=1)
            found.append((dot_nt(query, keys), values))
        return found

    def fold(part):
        halves = [part[i * rows : (i + 1) * rows] for i in range(2)]
        return jnp.concatenate([half + pltpu.roll(half, heads, 0) for half in halves], axis=0)

    def finish(step, found):
        for b in range(0, block, 2):
            s = step * block + b
            length = jnp.where(second, lengths_ref[s + 1], lengths_ref[s])
            scores = jnp.where(position < length, found[b // 2][0] * scaling, neg_fill)
            fresh = jnp.sum(q_scr[s : s + 2] * k_scr[s : s + 2][:, None, :], axis=2, keepdims=True)
            fresh = fresh.reshape(2 * rows, 1) * scaling
            top = jnp.maximum(jnp.max(scores, axis=1, keepdims=True), fresh)
            expo = jnp.exp(scores - top)
            expo_new = jnp.exp(fresh - top)
            factor = sign / (jnp.sum(expo, axis=1, keepdims=True) + expo_new)
            part_new = jnp.broadcast_to(expo_new * factor, (2 * rows, lanes))
            weights = fold(expo * factor).astype(bf16)
            weight_new = fold(part_new).astype(bf16).astype(f32)
            mixed = dot(weights, found[b // 2][1]).reshape(2, rows, lanes)
            o_scr[s : s + 2] = (
                mixed + weight_new.reshape(2, rows, lanes) * v_scr[s : s + 2][:, None, :]
            )

    held = None
    for step in range(steps + 1):
        if step < steps:
            streams[step].wait()
            found = scores_of(step)
        if step:
            finish(step - 1, held)
        held = found

    outs = []
    for h in range(heads):
        mix = jnp.where(own_keys, 0.0, o_scr[:, h, :])
        mean = jnp.sum(mix * mix, axis=1, keepdims=True) * (1.0 / v_width)
        mix = mix * lax.rsqrt(mean + epsilon)
        outs.append(mix + pltpu.roll(mix, v_width, 1))
    gains = jnp.concatenate([head_gain_ref[...], head_gain_ref[...]], axis=1)
    pairs = [
        jnp.where(upper, outs[2 * p + 1], outs[2 * p]) * gains for p in range(heads // 2)
    ]
    head_out = jnp.concatenate(pairs, axis=1).astype(bf16)
    heads_ref[...] = head_out
    mix_scr[...] = dot(picks, head_out).astype(bf16)
    backs[1].start()
    for back in backs:
        back.wait()


def silu(values):
    return values / (1.0 + jnp.exp(-values))


def partner(index, d, count):
    return index ^ d if count & (count - 1) == 0 else (index + d) % count


def own_kernel(
    capacity,
    experts,
    kept,
    heads_ref,
    w_out_hbm,
    tokens_hbm,
    gain_hbm,
    s_gate_hbm,
    s_up_hbm,
    s_down_hbm,
    routing_hbm,
    rates_hbm,
    *refs,
):
    tp_count, seqs, width = heads_ref.shape
    part_refs = refs[: tp_count - 1]
    base_ref, mix_ref, gain_ref, *kept_refs = refs[tp_count - 1 : tp_count + 2 + kept]
    refs = refs[tp_count + 2 + kept :]
    (
        tokens_ref,
        rest_ref,
        s_gate_ref,
        s_up_ref,
        s_down_ref,
        routing_ref,
        rates_ref,
        res_scr,
        slot_scr,
        sems,
    ) = refs
    share = base_ref.shape[1]
    blocks = column_blocks(w_out_hbm, rest_ref, kept_refs)
    early = [
        (tokens_hbm, tokens_ref),
        (gain_hbm, gain_ref),
        (routing_hbm, routing_ref),
        (rates_hbm, rates_ref),
        *blocks,
        (s_gate_hbm, s_gate_ref),
        (s_up_hbm, s_up_ref),
        (s_down_hbm, s_down_ref),
    ]
    copies = [
        pltpu.make_async_copy(source, target, sems.at[i])
        for i, (source, target) in enumerate(early)
    ]
    for copy in copies:
        copy.start()
    for copy in copies[:4]:
        copy.wait()
    slots = own_slots(routing_ref, slot_scr, seqs, experts, capacity)
    top_count = rates_ref.shape[0]
    rates = jnp.concatenate([rates_ref[...], jnp.zeros((8 - top_count, seqs), f32)], axis=0)
    rates = jnp.concatenate([rates, jnp.zeros((8, 128 - seqs), f32)], axis=1).T[:seqs]
    ids = iota((seqs, experts * capacity), 1)
    mixing = jnp.zeros((seqs, experts * capacity), f32)
    for k, slot in enumerate(slots):
        mixing = jnp.where(slot == ids, rates[:, k : k + 1], mixing)
    high = mixing.astype(bf16)
    mix_ref[:seqs] = high
    mix_ref[seqs:] = (mixing - high.astype(f32)).astype(bf16)

    square = jnp.zeros((seqs, 1), f32)
    for n in range(tp_count):
        copies[4 + n].wait()
        w_out_ref = blocks[n][1]
        cut = slice(n * share, (n + 1) * share)
        total = tokens_ref[:, cut].astype(f32)
        parts = jnp.zeros((seqs, share), f32)
        for j in range(tp_count):
            part = dot(heads_ref[j], w_out_ref[j * width : (j + 1) * width])
            parts = parts + part.astype(bf16).astype(f32)
        residual = (total + parts).astype(bf16).astype(f32)
        res_scr[:, cut] = residual
        square = square + jnp.sum(residual * residual, axis=1, keepdims=True)
    scale = lax.rsqrt(square * (1.0 / res_scr.shape[1]) + epsilon)
    ffn_in = (res_scr[...] * scale * gain_ref[...]).astype(bf16)
    for copy in copies[4 + tp_count :]:
        copy.wait()
    act = silu(dot(ffn_in, s_gate_ref[...])) * dot(ffn_in, s_up_ref[...])
    act = act.astype(bf16)
    for d in range(tp_count):
        start = pl.multiple_of(partner(lax.axis_index("tp"), d, tp_count) * share, share)
        part = dot(act, s_down_ref[:, pl.ds(start, share)])
        if d:
            part_refs[d - 1][...] = part.astype(bf16)
        else:
            base_ref[...] = res_scr[:, pl.ds(start, share)] + part


def column_blocks(w_out_hbm, rest_ref, kept_refs):
    share = rest_ref.shape[2]
    targets = [*kept_refs, *[rest_ref.at[i] for i in range(rest_ref.shape[0])]]
    return [
        (w_out_hbm.at[:, pl.ds(n * share, share)], target) for n, target in enumerate(targets)
    ]


def expert_kernel(
    direct,
    kept,
    arrived_ref,
    gain_ref,
    *refs,
):
    kept_refs = refs[:kept]
    (
        w_out_hbm,
        gate_hbm,
        up_hbm,
        down_hbm,
        send_hbm,
        send_ref,
        rest_ref,
        gate_ref,
        up_ref,
        down_ref,
        res_scr,
        sems,
    ) = refs[kept:]
    blocks = column_blocks(w_out_hbm, rest_ref, kept_refs)
    copies = [
        pltpu.make_async_copy(source, target, sems.at[i])
        for i, (source, target) in enumerate(
            [
                *blocks[kept:],
                (gate_hbm, gate_ref),
                (up_hbm, up_ref),
                *column_blocks(down_hbm, down_ref, ()),
            ]
        )
    ]
    for copy in copies:
        copy.start()
    groups, chunk, packed = arrived_ref.shape
    rows, model = res_scr.shape
    capacity = rows // groups
    tp_count = chunk // capacity
    share = model // tp_count
    width = packed - share
    lefts = []
    tokens = []
    for j in range(tp_count):
        piece = arrived_ref[:, j * capacity : (j + 1) * capacity, :].astype(f32)
        piece = piece.reshape(rows, packed)
        lefts.append(piece[:, :width].astype(bf16))
        tokens.append(piece[:, width:])
    square = jnp.zeros((rows, 1), f32)
    for n in range(tp_count):
        if n >= kept:
            copies[n - kept].wait()
        w_out_ref = blocks[n][1]
        cut = slice(n * share, (n + 1) * share)
        total = jnp.zeros((rows, share), f32)
        for j in range(tp_count):
            part = dot(lefts[j], w_out_ref[j * width : (j + 1) * width])
            total = total + part.astype(bf16).astype(f32)
        residual = (tokens[n] + total).astype(bf16).astype(f32)
        res_scr[:, cut] = residual
        square = square + jnp.sum(residual * residual, axis=1, keepdims=True)
    scale = lax.rsqrt(square * (1.0 / model) + epsilon)
    ffn_in = (res_scr[...] * scale * gain_ref[...]).astype(bf16)
    copies[tp_count - kept].wait()
    gate = dot(ffn_in, gate_ref[...])
    copies[tp_count - kept + 1].wait()
    act = (silu(gate) * dot(ffn_in, up_ref[...])).astype(bf16)
    for n in range(tp_count):
        copies[n - tp_count].wait()
        result = dot(act, down_ref[n])
        if direct:
            for i in range(groups):
                first = (i * tp_count + n) * capacity
                send_ref[first : first + capacity, :] = result[
                    i * capacity : (i + 1) * capacity
                ].astype(bf16)
        else:
            send_ref[:, n * share : (n + 1) * share] = result.astype(bf16)
    back = pltpu.make_async_copy(send_ref, send_hbm, sems.at[0])
    back.start()
    back.wait()


def combine_kernel(base_ref, mix_ref, returned_ref, *refs):
    *part_refs, out_ref = refs
    seqs = out_ref.shape[0]
    returned = returned_ref[...]
    routed = dot(mix_ref[...], returned)
    shared = base_ref[...]
    for part_ref in part_refs:
        shared = shared + part_ref[...].astype(f32)
    out_ref[...] = (shared + routed[:seqs] + routed[seqs:]).astype(bf16)


def params(mib, **more):
    return pltpu.CompilerParams(vmem_limit_bytes=mib << 20, **more)


def shards(
    tokens,
    kv_cache,
    lengths,
    attn_gain,
    w_query,
    w_key,
    w_value,
    lambdas,
    head_gain,
    w_out,
    ffn_gain,
    w_shared_gate,
    w_shared_up,
    w_shared_down,
    routing,
    route_weights,
    w_exp_gate,
    w_exp_up,
    w_exp_down,
):
    seqs, width = tokens.shape
    tp_count = lax.axis_size("tp")
    ep_count = lax.axis_size("ep")
    devices = ep_count * tp_count
    top_count = routing.shape[1]
    experts = w_exp_gate.shape[0] * devices
    capacity = max(2, 2 * seqs * top_count // experts)
    cache_len, lanes = kv_cache.shape[1:]
    v_width = head_gain.shape[0]
    heads = lambdas.shape[0]
    share = width // tp_count
    local = heads * v_width
    packed = local + share
    direct = capacity % 8 == 0
    block = 4
    head_out, send = pl.pallas_call(
        functools.partial(attention_kernel, capacity, experts, block),
        in_specs=[HBM] * 10,
        out_specs=[VMEM, HBM],
        out_shape=[
            pltpu.VMEM((seqs, local), bf16),
            jax.ShapeDtypeStruct((devices * capacity, packed), bf16),
        ],
        scratch_shapes=[
            pltpu.VMEM(tokens.shape, bf16),
            pltpu.VMEM((1, width), f32),
            pltpu.VMEM(w_query.shape, bf16),
            pltpu.VMEM(w_key.shape[::-1], bf16),
            pltpu.VMEM(w_value.shape[::-1], bf16),
            pltpu.VMEM((1, v_width), f32),
            pltpu.VMEM(routing.shape[::-1], jnp.int32),
            pltpu.SMEM(lengths.shape, jnp.int32),
            pltpu.SMEM(lambdas.shape, f32),
            pltpu.VMEM(kv_cache.shape, bf16),
            pltpu.VMEM((seqs, 2 * heads, lanes), f32),
            pltpu.VMEM((seqs, lanes), f32),
            pltpu.VMEM((seqs, lanes), f32),
            pltpu.VMEM((seqs, 2 * heads, lanes), f32),
            pltpu.VMEM((routing.shape[0], 8), f32),
            pltpu.VMEM((devices * capacity, share), bf16),
            pltpu.VMEM((devices * capacity, local), bf16),
            pltpu.SemaphoreType.DMA((9,)),
            pltpu.SemaphoreType.DMA((seqs // block,)),
            pltpu.SemaphoreType.DMA((2,)),
        ],
        compiler_params=pltpu.CompilerParams(vmem_limit_bytes=67_043_328 - 2 * seqs * local),
        cost_estimate=pl.CostEstimate(
            flops=seqs * cache_len * lanes * 32, bytes_accessed=kv_cache.size * 2, transcendentals=0
        ),
        name="attention",
    )(
        tokens,
        attn_gain.reshape(1, width),
        w_query,
        w_key.T,
        w_value.T,
        head_gain.reshape(1, v_width),
        routing.T,
        lengths,
        lambdas,
        kv_cache,
    )

    arrived = lax.all_to_all(send, ("ep", "tp"), split_axis=0, concat_axis=0, tiled=True)
    arrived = arrived.reshape(ep_count, tp_count * capacity, packed)
    all_heads = lax.all_gather(head_out, "tp", axis=0, tiled=False)

    exp_gate = w_exp_gate.reshape(w_exp_gate.shape[1:])
    exp_up = w_exp_up.reshape(w_exp_up.shape[1:])
    exp_down = w_exp_down.reshape(w_exp_down.shape[1:])
    rows = ep_count * capacity
    slot_count = experts * capacity
    kept = 1
    w_out_block = (w_out.shape[0], share)
    rest = pltpu.VMEM((tp_count - kept, *w_out_block), bf16)
    results = pl.pallas_call(
        functools.partial(own_kernel, capacity, experts, kept),
        in_specs=[VMEM] + [HBM] * 8,
        out_specs=[VMEM] * (tp_count + 2 + kept),
        out_shape=[pltpu.VMEM((seqs, share), bf16)] * (tp_count - 1)
        + [
            pltpu.VMEM((seqs, share), f32),
            pltpu.VMEM((2 * seqs, slot_count), bf16),
            pltpu.VMEM((1, width), f32),
        ]
        + [pltpu.VMEM(w_out_block, bf16)] * kept,
        scratch_shapes=[
            pltpu.VMEM(tokens.shape, bf16),
            rest,
            pltpu.VMEM(w_shared_gate.shape, bf16),
            pltpu.VMEM(w_shared_up.shape, bf16),
            pltpu.VMEM(w_shared_down.shape, bf16),
            pltpu.VMEM(routing.shape[::-1], jnp.int32),
            pltpu.VMEM(route_weights.shape[::-1], f32),
            pltpu.VMEM((seqs, width), f32),
            pltpu.VMEM((routing.shape[0], 8), f32),
            pltpu.SemaphoreType.DMA((7 + tp_count,)),
        ],
        compiler_params=pltpu.CompilerParams(vmem_limit_bytes=63_900_000),
        cost_estimate=pl.CostEstimate(
            flops=2 * seqs * w_out.size, bytes_accessed=12 << 20, transcendentals=0
        ),
        name="own",
    )(
        all_heads,
        w_out,
        tokens,
        ffn_gain.reshape(1, width),
        w_shared_gate,
        w_shared_up,
        w_shared_down,
        routing.T,
        route_weights.T,
    )

    part, (base, mix, gain), kept_blocks = (
        results[: tp_count - 1],
        results[tp_count - 1 : tp_count + 2],
        results[tp_count + 2 :],
    )
    arrived, gain, *kept_blocks = [
        pltpu.with_memory_space_constraint(value, pltpu.VMEM)
        for value in (arrived, gain, *kept_blocks)
    ]
    sent_shape = (devices * capacity, share) if direct else (rows, width)
    sent = pl.pallas_call(
        functools.partial(expert_kernel, direct, kept),
        in_specs=[VMEM] * (2 + kept) + [HBM] * 4,
        out_specs=HBM,
        out_shape=jax.ShapeDtypeStruct(sent_shape, bf16),
        scratch_shapes=[
            pltpu.VMEM(sent_shape, bf16),
            rest,
            pltpu.VMEM(exp_gate.shape, bf16),
            pltpu.VMEM(exp_up.shape, bf16),
            pltpu.VMEM((tp_count, exp_down.shape[0], share), bf16),
            pltpu.VMEM((rows, width), f32),
            pltpu.SemaphoreType.DMA((2 + 2 * tp_count - kept,)),
        ],
        compiler_params=pltpu.CompilerParams(vmem_limit_bytes=60 * 1024 * 1024),
        cost_estimate=pl.CostEstimate(
            flops=2 * rows * 5 * w_out.size // 2, bytes_accessed=1 << 20, transcendentals=0
        ),
        name="experts",
    )(arrived, gain, *kept_blocks, w_out, exp_gate, exp_up, exp_down)
    if not direct:
        sent = sent.reshape(ep_count, capacity, tp_count, share)
        sent = sent.transpose(0, 2, 1, 3).reshape(devices * capacity, share)
    returned = lax.all_to_all(sent, ("ep", "tp"), split_axis=0, concat_axis=0, tiled=True)
    parts = [
        lax.ppermute(piece, "tp", [(i, partner(i, d, tp_count)) for i in range(tp_count)])
        for d, piece in enumerate(part, 1)
    ]

    return pl.pallas_call(
        combine_kernel,
        in_specs=[VMEM] * (tp_count + 2),
        out_specs=VMEM,
        out_shape=jax.ShapeDtypeStruct((seqs, share), bf16),
        compiler_params=params(16),
        name="combine",
    )(base, mix, returned, *parts)


def solution(mesh):
    return jax.shard_map(
        shards,
        mesh=mesh,
        in_specs=(
            P("ep", None),
            P("ep", None, "tp"),
            P("ep"),
            P(),
            P(None, "tp"),
            P(None, "tp"),
            P(None, "tp"),
            P("tp"),
            P(),
            P(),
            P(),
            P(None, "tp"),
            P(None, "tp"),
            P("tp", None),
            P(),
            P("ep", None),
            P(("ep", "tp"), None, None),
            P(("ep", "tp"), None, None),
            P(("ep", "tp"), None, None),
        ),
        out_specs=P("ep", "tp"),
        check_vma=False,
    )
```

```python
import functools

import jax
import jax.numpy as jnp
from jax import lax
from jax.experimental import pallas as pl
from jax.experimental.pallas import tpu as pltpu
from jax.sharding import PartitionSpec as P


epsilon = 1e-06
neg_fill = -1e30
f32 = jnp.float32
bf16 = jnp.bfloat16
VMEM = pl.BlockSpec(memory_space=pltpu.VMEM)
SMEM = pl.BlockSpec(memory_space=pltpu.SMEM)
HBM = pl.BlockSpec(memory_space=pltpu.HBM)


def iota(shape, axis):
    return lax.broadcasted_iota(jnp.int32, shape, axis)


def dot(a, b):
    return jnp.dot(a, b, preferred_element_type=f32)


def dot_nt(a, b):
    return lax.dot_general(a, b, (((1,), (1,)), ((), ())), preferred_element_type=f32)


def inv_rms(values):
    return lax.rsqrt(jnp.mean(values * values, axis=-1, keepdims=True) + epsilon)


def slots_of(routing, experts, capacity):
    rows, top_count = routing.shape
    ids = iota((rows, experts), 1)
    hits = [routing[:, k : k + 1] == ids for k in range(top_count)]
    present = jnp.zeros((rows, experts), f32)
    for hit in hits:
        present = jnp.where(hit, 1.0, present)
    earlier = (iota((rows, rows), 1) < iota((rows, rows), 0)).astype(bf16)
    before = dot(earlier, present.astype(bf16))
    ranks = [jnp.sum(jnp.where(hit, before, 0.0), axis=1, keepdims=True) for hit in hits]
    return [
        routing[:, k : k + 1] * capacity + ranks[k].astype(jnp.int32) for k in range(top_count)
    ]


def own_slots(routing_ref, slot_scr, seqs, experts, capacity):
    top_count, batch = routing_ref.shape
    pad = jnp.zeros((8 - top_count, batch), f32)
    slot_scr[...] = jnp.concatenate([routing_ref[...].astype(f32), pad], axis=0).T
    start = pl.multiple_of(lax.axis_index("ep") * seqs, seqs)
    own = slot_scr[pl.ds(start, seqs), :top_count].astype(jnp.int32)
    return slots_of(own, experts, capacity)


def attention_kernel(
    capacity,
    experts,
    block,
    tokens_hbm,
    attn_gain_hbm,
    w_query_hbm,
    w_key_hbm,
    w_value_hbm,
    head_gain_hbm,
    routing_hbm,
    lengths_hbm,
    lambdas_hbm,
    kv_hbm,
    heads_ref,
    send_hbm,
    tokens_ref,
    attn_gain_ref,
    w_query_ref,
    w_key_ref,
    w_value_ref,
    head_gain_ref,
    routing_ref,
    lengths_ref,
    lambdas_ref,
    kv_ref,
    q_scr,
    k_scr,
    v_scr,
    o_scr,
    slot_scr,
    back_scr,
    mix_scr,
    sems,
    kv_sems,
    back_sems,
):
    seqs, rows, lanes = q_scr.shape
    heads = rows // 2
    v_width = lanes // 2
    qk_width = v_width // 2
    cache_len = kv_ref.shape[1]
    width = mix_scr.shape[1]
    share = back_scr.shape[1]
    scaling = qk_width ** (-0.5)
    copies = [
        pltpu.make_async_copy(source, target, sems.at[i])
        for i, (source, target) in enumerate(
            [
                (tokens_hbm, tokens_ref),
                (attn_gain_hbm, attn_gain_ref),
                (routing_hbm, routing_ref),
                (w_query_hbm, w_query_ref),
                (w_key_hbm, w_key_ref),
                (w_value_hbm, w_value_ref),
                (lengths_hbm, lengths_ref),
                (lambdas_hbm, lambdas_ref),
                (head_gain_hbm, head_gain_ref),
            ]
        )
    ]
    for copy in copies:
        copy.start()
    steps = seqs // block
    streams = [
        pltpu.make_async_copy(
            kv_hbm.at[pl.ds(i * block, block)], kv_ref.at[pl.ds(i * block, block)], kv_sems.at[i]
        )
        for i in range(steps)
    ]
    streams[0].start()
    for copy in copies[:3]:
        copy.wait()
    for stream in streams[1:]:
        stream.start()

    slots = own_slots(routing_ref, slot_scr, seqs, experts, capacity)
    ids = iota((seqs, experts * capacity), 1)
    picks = jnp.zeros((seqs, experts * capacity), f32)
    for slot in slots:
        picks = jnp.where(slot == ids, 1.0, picks)
    picks = picks.T.astype(bf16)
    start = pl.multiple_of(lax.axis_index("tp") * share, share)
    back_scr[...] = dot(picks, tokens_ref[:, pl.ds(start, share)]).astype(bf16)
    backs = [
        pltpu.make_async_copy(back_scr, send_hbm.at[:, pl.ds(width, share)], back_sems.at[0]),
        pltpu.make_async_copy(mix_scr, send_hbm.at[:, pl.ds(0, width)], back_sems.at[1]),
    ]
    backs[0].start()
    tokens = tokens_ref[...].astype(f32)
    normed = (tokens * inv_rms(tokens) * attn_gain_ref[...]).astype(bf16)

    for copy in copies[3:]:
        copy.wait()
    queries = dot(normed, w_query_ref[...]).astype(bf16).astype(f32)
    key_new = dot_nt(normed, w_key_ref[...]).astype(bf16).astype(f32)
    value_new = dot_nt(normed, w_value_ref[...]).astype(bf16).astype(f32)
    k_scr[...] = jnp.concatenate([key_new, key_new], axis=1)
    v_scr[...] = jnp.concatenate([value_new, value_new], axis=1)
    lane = iota((seqs, lanes), 1)
    upper = lane >= v_width
    own_keys = upper == (iota((seqs, lanes), 0) % 2 == 1)
    for h in range(heads):
        pair = queries[:, (h // 2) * lanes : (h // 2 + 1) * lanes]
        pair = jnp.where(upper == (h % 2 == 1), pair, pltpu.roll(pair, v_width, 1))
        for m in range(2):
            inner = lane % v_width
            keep = own_keys & (inner >= m * qk_width) & (inner < (m + 1) * qk_width)
            q_scr[:, m * heads + h, :] = jnp.where(keep, pair, 0.0)

    row = iota((2 * rows, 1), 0)
    sign = jnp.where(row < rows, 1.0, 0.0)
    for h in range(heads):
        sign = jnp.where((row >= rows) & (row % heads == h), -lambdas_ref[h], sign)
    position = iota((2 * rows, cache_len), 1)
    second = row % rows >= heads

    def query_of(s):
        even, odd = q_scr[s], q_scr[s + 1]
        return jnp.concatenate([even[:heads], odd[:heads], even[heads:], odd[heads:]], axis=0)

    def scores_of(step):
        found = []
        for b in range(0, block, 2):
            s = step * block + b
            even, odd = kv_ref[s], kv_ref[s + 1]
            query = query_of(s)
            keys = jnp.concatenate([even[:, :v_width], odd[:, :v_width]], axis=1)
            values = jnp.concatenate([odd[:, v_width:], even[:, v_width:]], axis=1)
            fresh = query * jnp.where(second, k_scr[s + 1 : s + 2], k_scr[s : s + 1])
            fresh = jnp.sum(fresh, axis=1, keepdims=True)
            found.append((dot_nt(query.astype(bf16), keys), fresh, values))
        return found

    def weights_of(step, found):
        made = []
        for b in range(0, block, 2):
            s = step * block + b
            scores, fresh, values = found[b // 2]
            length = jnp.where(second, lengths_ref[s + 1], lengths_ref[s])
            scores = jnp.where(position < length, scores * scaling, neg_fill)
            fresh = fresh * scaling
            top = jnp.maximum(jnp.max(scores, axis=1, keepdims=True), fresh)
            expo = jnp.exp(scores - top)
            expo_new = jnp.exp(fresh - top)
            factor = sign / (jnp.sum(expo, axis=1, keepdims=True) + expo_new)
            part = expo * factor
            part_new = expo_new * factor
            weights = (part[:rows] + part[rows:]).astype(bf16)
            weight_new = (part_new[:rows] + part_new[rows:]).astype(bf16).astype(f32)
            value_new = jnp.where(second[:rows], v_scr[s + 1 : s + 2], v_scr[s : s + 1])
            made.append((weights, weight_new * value_new, values))
        return made

    def mix_values(step, made):
        for b in range(0, block, 2):
            weights, newest, values = made[b // 2]
            o_scr[(step * block + b) // 2] = dot(weights, values) + newest

    found, made = None, None
    for step in range(steps + 2):
        if step < steps:
            streams[step].wait()
        if step >= 2:
            mix_values(step - 2, made)
        if 1 <= step <= steps:
            made = weights_of(step - 1, found)
        if step < steps:
            found = scores_of(step)

    gains = jnp.concatenate([head_gain_ref[...], head_gain_ref[...]], axis=1)
    half = upper[: seqs // 2]
    for i in range(2):
        outs = []
        for h in range(heads):
            mix = jnp.where(half == (i == 0), o_scr[:, i * heads + h, :], 0.0)
            mean = jnp.sum(mix * mix, axis=1, keepdims=True) * (1.0 / v_width)
            mix = mix * lax.rsqrt(mean + epsilon)
            turned = pltpu.roll(mix, v_width, 1)
            outs.append((turned, mix) if i == 0 else (mix, turned))
        for p in range(heads // 2):
            out = jnp.where(half, outs[2 * p + 1][1], outs[2 * p][0]) * gains
            q_scr[i :: 2, p, :] = out
    head_out = jnp.concatenate([q_scr[:, p, :] for p in range(heads // 2)], axis=1).astype(bf16)
    heads_ref[...] = head_out
    mix_scr[...] = dot(picks, head_out).astype(bf16)
    backs[1].start()
    for back in backs:
        back.wait()


def silu(values):
    return values / (1.0 + jnp.exp(-values))


def partner(index, d, count):
    return index ^ d if count & (count - 1) == 0 else (index + d) % count


def own_kernel(
    capacity,
    experts,
    kept,
    heads_ref,
    w_out_hbm,
    tokens_hbm,
    gain_hbm,
    s_gate_hbm,
    s_up_hbm,
    s_down_hbm,
    routing_hbm,
    rates_hbm,
    *refs,
):
    tp_count, seqs, width = heads_ref.shape
    part_refs = refs[: tp_count - 1]
    base_ref, mix_ref, gain_ref, *kept_refs = refs[tp_count - 1 : tp_count + 2 + kept]
    refs = refs[tp_count + 2 + kept :]
    (
        tokens_ref,
        rest_ref,
        s_gate_ref,
        s_up_ref,
        s_down_ref,
        routing_ref,
        rates_ref,
        res_scr,
        slot_scr,
        sems,
    ) = refs
    share = base_ref.shape[1]
    blocks = column_blocks(w_out_hbm, rest_ref, kept_refs)
    early = [
        (tokens_hbm, tokens_ref),
        (gain_hbm, gain_ref),
        (routing_hbm, routing_ref),
        (rates_hbm, rates_ref),
        *blocks,
        (s_gate_hbm, s_gate_ref),
        (s_up_hbm, s_up_ref),
        (s_down_hbm, s_down_ref),
    ]
    copies = [
        pltpu.make_async_copy(source, target, sems.at[i])
        for i, (source, target) in enumerate(early)
    ]
    for copy in copies:
        copy.start()
    for copy in copies[:4]:
        copy.wait()
    slots = own_slots(routing_ref, slot_scr, seqs, experts, capacity)
    top_count = rates_ref.shape[0]
    rates = jnp.concatenate([rates_ref[...], jnp.zeros((8 - top_count, seqs), f32)], axis=0)
    rates = jnp.concatenate([rates, jnp.zeros((8, 128 - seqs), f32)], axis=1).T[:seqs]
    ids = iota((seqs, experts * capacity), 1)
    mixing = jnp.zeros((seqs, experts * capacity), f32)
    for k, slot in enumerate(slots):
        mixing = jnp.where(slot == ids, rates[:, k : k + 1], mixing)
    high = mixing.astype(bf16)
    mix_ref[:seqs] = high
    mix_ref[seqs:] = (mixing - high.astype(f32)).astype(bf16)

    square = jnp.zeros((seqs, 1), f32)
    for n in range(tp_count):
        copies[4 + n].wait()
        w_out_ref = blocks[n][1]
        cut = slice(n * share, (n + 1) * share)
        total = tokens_ref[:, cut].astype(f32)
        parts = jnp.zeros((seqs, share), f32)
        for j in range(tp_count):
            part = dot(heads_ref[j], w_out_ref[j * width : (j + 1) * width])
            parts = parts + part.astype(bf16).astype(f32)
        residual = (total + parts).astype(bf16).astype(f32)
        res_scr[:, cut] = residual
        square = square + jnp.sum(residual * residual, axis=1, keepdims=True)
    scale = lax.rsqrt(square * (1.0 / res_scr.shape[1]) + epsilon)
    ffn_in = (res_scr[...] * scale * gain_ref[...]).astype(bf16)
    for copy in copies[4 + tp_count :]:
        copy.wait()
    act = silu(dot(ffn_in, s_gate_ref[...])) * dot(ffn_in, s_up_ref[...])
    act = act.astype(bf16)
    for d in range(tp_count):
        start = pl.multiple_of(partner(lax.axis_index("tp"), d, tp_count) * share, share)
        part = dot(act, s_down_ref[:, pl.ds(start, share)])
        if d:
            part_refs[d - 1][...] = part.astype(bf16)
        else:
            base_ref[...] = res_scr[:, pl.ds(start, share)] + part


def column_blocks(w_out_hbm, rest_ref, kept_refs):
    share = rest_ref.shape[2]
    targets = [*kept_refs, *[rest_ref.at[i] for i in range(rest_ref.shape[0])]]
    return [
        (w_out_hbm.at[:, pl.ds(n * share, share)], target) for n, target in enumerate(targets)
    ]


def expert_kernel(
    direct,
    kept,
    arrived_ref,
    gain_ref,
    *refs,
):
    kept_refs = refs[:kept]
    (
        w_out_hbm,
        gate_hbm,
        up_hbm,
        down_hbm,
        send_hbm,
        send_ref,
        rest_ref,
        gate_ref,
        up_ref,
        down_ref,
        res_scr,
        sems,
    ) = refs[kept:]
    blocks = column_blocks(w_out_hbm, rest_ref, kept_refs)
    copies = [
        pltpu.make_async_copy(source, target, sems.at[i])
        for i, (source, target) in enumerate(
            [
                *blocks[kept:],
                (gate_hbm, gate_ref),
                (up_hbm, up_ref),
                *column_blocks(down_hbm, down_ref, ()),
            ]
        )
    ]
    for copy in copies:
        copy.start()
    groups, chunk, packed = arrived_ref.shape
    rows, model = res_scr.shape
    capacity = rows // groups
    tp_count = chunk // capacity
    share = model // tp_count
    width = packed - share
    lefts = []
    tokens = []
    for j in range(tp_count):
        piece = arrived_ref[:, j * capacity : (j + 1) * capacity, :].astype(f32)
        piece = piece.reshape(rows, packed)
        lefts.append(piece[:, :width].astype(bf16))
        tokens.append(piece[:, width:])
    square = jnp.zeros((rows, 1), f32)
    for n in range(tp_count):
        if n >= kept:
            copies[n - kept].wait()
        w_out_ref = blocks[n][1]
        cut = slice(n * share, (n + 1) * share)
        total = jnp.zeros((rows, share), f32)
        for j in range(tp_count):
            part = dot(lefts[j], w_out_ref[j * width : (j + 1) * width])
            total = total + part.astype(bf16).astype(f32)
        residual = (tokens[n] + total).astype(bf16).astype(f32)
        res_scr[:, cut] = residual
        square = square + jnp.sum(residual * residual, axis=1, keepdims=True)
    scale = lax.rsqrt(square * (1.0 / model) + epsilon)
    ffn_in = (res_scr[...] * scale * gain_ref[...]).astype(bf16)
    copies[tp_count - kept].wait()
    gate = dot(ffn_in, gate_ref[...])
    copies[tp_count - kept + 1].wait()
    act = (silu(gate) * dot(ffn_in, up_ref[...])).astype(bf16)
    for n in range(tp_count):
        copies[n - tp_count].wait()
        result = dot(act, down_ref[n])
        if direct:
            for i in range(groups):
                first = (i * tp_count + n) * capacity
                send_ref[first : first + capacity, :] = result[
                    i * capacity : (i + 1) * capacity
                ].astype(bf16)
        else:
            send_ref[:, n * share : (n + 1) * share] = result.astype(bf16)
    back = pltpu.make_async_copy(send_ref, send_hbm, sems.at[0])
    back.start()
    back.wait()


def combine_kernel(base_ref, mix_ref, returned_ref, *refs):
    *part_refs, out_ref = refs
    seqs = out_ref.shape[0]
    returned = returned_ref[...]
    routed = dot(mix_ref[...], returned)
    shared = base_ref[...]
    for part_ref in part_refs:
        shared = shared + part_ref[...].astype(f32)
    out_ref[...] = (shared + routed[:seqs] + routed[seqs:]).astype(bf16)


def params(mib, **more):
    return pltpu.CompilerParams(vmem_limit_bytes=mib << 20, **more)


def shards(
    tokens,
    kv_cache,
    lengths,
    attn_gain,
    w_query,
    w_key,
    w_value,
    lambdas,
    head_gain,
    w_out,
    ffn_gain,
    w_shared_gate,
    w_shared_up,
    w_shared_down,
    routing,
    route_weights,
    w_exp_gate,
    w_exp_up,
    w_exp_down,
):
    seqs, width = tokens.shape
    tp_count = lax.axis_size("tp")
    ep_count = lax.axis_size("ep")
    devices = ep_count * tp_count
    top_count = routing.shape[1]
    experts = w_exp_gate.shape[0] * devices
    capacity = max(2, 2 * seqs * top_count // experts)
    cache_len, lanes = kv_cache.shape[1:]
    v_width = head_gain.shape[0]
    heads = lambdas.shape[0]
    share = width // tp_count
    local = heads * v_width
    packed = local + share
    direct = capacity % 8 == 0
    block = 4
    head_out, send = pl.pallas_call(
        functools.partial(attention_kernel, capacity, experts, block),
        in_specs=[HBM] * 10,
        out_specs=[VMEM, HBM],
        out_shape=[
            pltpu.VMEM((seqs, local), bf16),
            jax.ShapeDtypeStruct((devices * capacity, packed), bf16),
        ],
        scratch_shapes=[
            pltpu.VMEM(tokens.shape, bf16),
            pltpu.VMEM((1, width), f32),
            pltpu.VMEM(w_query.shape, bf16),
            pltpu.VMEM(w_key.shape[::-1], bf16),
            pltpu.VMEM(w_value.shape[::-1], bf16),
            pltpu.VMEM((1, v_width), f32),
            pltpu.VMEM(routing.shape[::-1], jnp.int32),
            pltpu.SMEM(lengths.shape, jnp.int32),
            pltpu.SMEM(lambdas.shape, f32),
            pltpu.VMEM(kv_cache.shape, bf16),
            pltpu.VMEM((seqs, 2 * heads, lanes), f32),
            pltpu.VMEM((seqs, lanes), f32),
            pltpu.VMEM((seqs, lanes), f32),
            pltpu.VMEM((seqs // 2, 2 * heads, lanes), f32),
            pltpu.VMEM((routing.shape[0], 8), f32),
            pltpu.VMEM((devices * capacity, share), bf16),
            pltpu.VMEM((devices * capacity, local), bf16),
            pltpu.SemaphoreType.DMA((9,)),
            pltpu.SemaphoreType.DMA((seqs // block,)),
            pltpu.SemaphoreType.DMA((2,)),
        ],
        compiler_params=pltpu.CompilerParams(vmem_limit_bytes=67_043_328 - 2 * seqs * local),
        cost_estimate=pl.CostEstimate(
            flops=seqs * cache_len * lanes * 32, bytes_accessed=kv_cache.size * 2, transcendentals=0
        ),
        name="attention",
    )(
        tokens,
        attn_gain.reshape(1, width),
        w_query,
        w_key.T,
        w_value.T,
        head_gain.reshape(1, v_width),
        routing.T,
        lengths,
        lambdas,
        kv_cache,
    )

    arrived = lax.all_to_all(send, ("ep", "tp"), split_axis=0, concat_axis=0, tiled=True)
    arrived = arrived.reshape(ep_count, tp_count * capacity, packed)
    all_heads = lax.all_gather(head_out, "tp", axis=0, tiled=False)

    exp_gate = w_exp_gate.reshape(w_exp_gate.shape[1:])
    exp_up = w_exp_up.reshape(w_exp_up.shape[1:])
    exp_down = w_exp_down.reshape(w_exp_down.shape[1:])
    rows = ep_count * capacity
    slot_count = experts * capacity
    kept = 1
    w_out_block = (w_out.shape[0], share)
    rest = pltpu.VMEM((tp_count - kept, *w_out_block), bf16)
    results = pl.pallas_call(
        functools.partial(own_kernel, capacity, experts, kept),
        in_specs=[VMEM] + [HBM] * 8,
        out_specs=[VMEM] * (tp_count + 2 + kept),
        out_shape=[pltpu.VMEM((seqs, share), bf16)] * (tp_count - 1)
        + [
            pltpu.VMEM((seqs, share), f32),
            pltpu.VMEM((2 * seqs, slot_count), bf16),
            pltpu.VMEM((1, width), f32),
        ]
        + [pltpu.VMEM(w_out_block, bf16)] * kept,
        scratch_shapes=[
            pltpu.VMEM(tokens.shape, bf16),
            rest,
            pltpu.VMEM(w_shared_gate.shape, bf16),
            pltpu.VMEM(w_shared_up.shape, bf16),
            pltpu.VMEM(w_shared_down.shape, bf16),
            pltpu.VMEM(routing.shape[::-1], jnp.int32),
            pltpu.VMEM(route_weights.shape[::-1], f32),
            pltpu.VMEM((seqs, width), f32),
            pltpu.VMEM((routing.shape[0], 8), f32),
            pltpu.SemaphoreType.DMA((7 + tp_count,)),
        ],
        compiler_params=pltpu.CompilerParams(vmem_limit_bytes=63_900_000),
        cost_estimate=pl.CostEstimate(
            flops=2 * seqs * w_out.size, bytes_accessed=12 << 20, transcendentals=0
        ),
        name="own",
    )(
        all_heads,
        w_out,
        tokens,
        ffn_gain.reshape(1, width),
        w_shared_gate,
        w_shared_up,
        w_shared_down,
        routing.T,
        route_weights.T,
    )

    part, (base, mix, gain), kept_blocks = (
        results[: tp_count - 1],
        results[tp_count - 1 : tp_count + 2],
        results[tp_count + 2 :],
    )
    arrived, gain, *kept_blocks = [
        pltpu.with_memory_space_constraint(value, pltpu.VMEM)
        for value in (arrived, gain, *kept_blocks)
    ]
    sent_shape = (devices * capacity, share) if direct else (rows, width)
    sent = pl.pallas_call(
        functools.partial(expert_kernel, direct, kept),
        in_specs=[VMEM] * (2 + kept) + [HBM] * 4,
        out_specs=HBM,
        out_shape=jax.ShapeDtypeStruct(sent_shape, bf16),
        scratch_shapes=[
            pltpu.VMEM(sent_shape, bf16),
            rest,
            pltpu.VMEM(exp_gate.shape, bf16),
            pltpu.VMEM(exp_up.shape, bf16),
            pltpu.VMEM((tp_count, exp_down.shape[0], share), bf16),
            pltpu.VMEM((rows, width), f32),
            pltpu.SemaphoreType.DMA((2 + 2 * tp_count - kept,)),
        ],
        compiler_params=pltpu.CompilerParams(vmem_limit_bytes=60 * 1024 * 1024),
        cost_estimate=pl.CostEstimate(
            flops=2 * rows * 5 * w_out.size // 2, bytes_accessed=1 << 20, transcendentals=0
        ),
        name="experts",
    )(arrived, gain, *kept_blocks, w_out, exp_gate, exp_up, exp_down)
    if not direct:
        sent = sent.reshape(ep_count, capacity, tp_count, share)
        sent = sent.transpose(0, 2, 1, 3).reshape(devices * capacity, share)
    returned = lax.all_to_all(sent, ("ep", "tp"), split_axis=0, concat_axis=0, tiled=True)
    parts = [
        lax.ppermute(piece, "tp", [(i, partner(i, d, tp_count)) for i in range(tp_count)])
        for d, piece in enumerate(part, 1)
    ]

    return pl.pallas_call(
        combine_kernel,
        in_specs=[VMEM] * (tp_count + 2),
        out_specs=VMEM,
        out_shape=jax.ShapeDtypeStruct((seqs, share), bf16),
        compiler_params=params(16),
        name="combine",
    )(base, mix, returned, *parts)


def solution(mesh):
    return jax.shard_map(
        shards,
        mesh=mesh,
        in_specs=(
            P("ep", None),
            P("ep", None, "tp"),
            P("ep"),
            P(),
            P(None, "tp"),
            P(None, "tp"),
            P(None, "tp"),
            P("tp"),
            P(),
            P(),
            P(),
            P(None, "tp"),
            P(None, "tp"),
            P("tp", None),
            P(),
            P("ep", None),
            P(("ep", "tp"), None, None),
            P(("ep", "tp"), None, None),
            P(("ep", "tp"), None, None),
        ),
        out_specs=P("ep", "tp"),
        check_vma=False,
    )
```

```python
import functools

import jax
import jax.numpy as jnp
from jax import lax
from jax.experimental import pallas as pl
from jax.experimental.pallas import tpu as pltpu
from jax.sharding import PartitionSpec as P


epsilon = 1e-06
neg_fill = -1e30
f32 = jnp.float32
bf16 = jnp.bfloat16
VMEM = pl.BlockSpec(memory_space=pltpu.VMEM)
SMEM = pl.BlockSpec(memory_space=pltpu.SMEM)
HBM = pl.BlockSpec(memory_space=pltpu.HBM)


def iota(shape, axis):
    return lax.broadcasted_iota(jnp.int32, shape, axis)


def dot(a, b):
    return jnp.dot(a, b, preferred_element_type=f32)


def dot_nt(a, b):
    return lax.dot_general(a, b, (((1,), (1,)), ((), ())), preferred_element_type=f32)


def inv_rms(values):
    return lax.rsqrt(jnp.mean(values * values, axis=-1, keepdims=True) + epsilon)


def slots_of(routing, experts, capacity):
    rows, top_count = routing.shape
    ids = iota((rows, experts), 1)
    hits = [routing[:, k : k + 1] == ids for k in range(top_count)]
    present = jnp.zeros((rows, experts), f32)
    for hit in hits:
        present = jnp.where(hit, 1.0, present)
    earlier = (iota((rows, rows), 1) < iota((rows, rows), 0)).astype(bf16)
    before = dot(earlier, present.astype(bf16))
    ranks = [jnp.sum(jnp.where(hit, before, 0.0), axis=1, keepdims=True) for hit in hits]
    return [
        routing[:, k : k + 1] * capacity + ranks[k].astype(jnp.int32) for k in range(top_count)
    ]


def own_slots(routing_ref, slot_scr, seqs, experts, capacity):
    top_count, batch = routing_ref.shape
    pad = jnp.zeros((8 - top_count, batch), f32)
    slot_scr[...] = jnp.concatenate([routing_ref[...].astype(f32), pad], axis=0).T
    start = pl.multiple_of(lax.axis_index("ep") * seqs, seqs)
    own = slot_scr[pl.ds(start, seqs), :top_count].astype(jnp.int32)
    return slots_of(own, experts, capacity)


def attention_kernel(
    capacity,
    experts,
    block,
    tokens_hbm,
    attn_gain_hbm,
    w_query_hbm,
    w_key_hbm,
    w_value_hbm,
    head_gain_hbm,
    routing_hbm,
    lengths_hbm,
    lambdas_hbm,
    kv_hbm,
    heads_ref,
    send_hbm,
    tokens_ref,
    attn_gain_ref,
    w_query_ref,
    w_key_ref,
    w_value_ref,
    head_gain_ref,
    routing_ref,
    lengths_ref,
    lambdas_ref,
    kv_ref,
    q_scr,
    k_scr,
    v_scr,
    o_scr,
    slot_scr,
    back_scr,
    mix_scr,
    sems,
    kv_sems,
    back_sems,
):
    seqs, rows, lanes = q_scr.shape
    heads = rows // 2
    v_width = lanes // 2
    qk_width = v_width // 2
    cache_len = kv_ref.shape[1]
    width = mix_scr.shape[1]
    share = back_scr.shape[1]
    scaling = qk_width ** (-0.5)
    copies = [
        pltpu.make_async_copy(source, target, sems.at[i])
        for i, (source, target) in enumerate(
            [
                (tokens_hbm, tokens_ref),
                (attn_gain_hbm, attn_gain_ref),
                (routing_hbm, routing_ref),
                (w_query_hbm, w_query_ref),
                (w_key_hbm, w_key_ref),
                (w_value_hbm, w_value_ref),
                (lengths_hbm, lengths_ref),
                (lambdas_hbm, lambdas_ref),
                (head_gain_hbm, head_gain_ref),
            ]
        )
    ]
    for copy in copies:
        copy.start()
    steps = seqs // block
    streams = [
        pltpu.make_async_copy(
            kv_hbm.at[pl.ds(i * block, block)], kv_ref.at[pl.ds(i * block, block)], kv_sems.at[i]
        )
        for i in range(steps)
    ]
    streams[0].start()
    for copy in copies[:3]:
        copy.wait()
    for stream in streams[1:]:
        stream.start()

    slots = own_slots(routing_ref, slot_scr, seqs, experts, capacity)
    ids = iota((seqs, experts * capacity), 1)
    picks = jnp.zeros((seqs, experts * capacity), f32)
    for slot in slots:
        picks = jnp.where(slot == ids, 1.0, picks)
    picks = picks.T.astype(bf16)
    start = pl.multiple_of(lax.axis_index("tp") * share, share)
    back_scr[...] = dot(picks, tokens_ref[:, pl.ds(start, share)]).astype(bf16)
    backs = [
        pltpu.make_async_copy(back_scr, send_hbm.at[:, pl.ds(width, share)], back_sems.at[0]),
        pltpu.make_async_copy(mix_scr, send_hbm.at[:, pl.ds(0, width)], back_sems.at[1]),
    ]
    backs[0].start()
    tokens = tokens_ref[...].astype(f32)
    normed = (tokens * inv_rms(tokens) * attn_gain_ref[...]).astype(bf16)

    for copy in copies[3:]:
        copy.wait()
    queries = dot(normed, w_query_ref[...]).astype(bf16).astype(f32)
    key_new = dot_nt(normed, w_key_ref[...]).astype(bf16).astype(f32)
    value_new = dot_nt(normed, w_value_ref[...]).astype(bf16).astype(f32)
    k_scr[...] = jnp.concatenate([key_new, key_new], axis=1)
    v_scr[...] = jnp.concatenate([value_new, value_new], axis=1)
    lane = iota((seqs, lanes), 1)
    upper = lane >= v_width
    own_keys = upper == (iota((seqs, lanes), 0) % 2 == 1)
    for h in range(heads):
        pair = queries[:, (h // 2) * lanes : (h // 2 + 1) * lanes]
        pair = jnp.where(upper == (h % 2 == 1), pair, pltpu.roll(pair, v_width, 1))
        for m in range(2):
            inner = lane % v_width
            keep = own_keys & (inner >= m * qk_width) & (inner < (m + 1) * qk_width)
            q_scr[:, m * heads + h, :] = jnp.where(keep, pair, 0.0)

    row = iota((2 * rows, 1), 0)
    sign = jnp.where(row < rows, 1.0, 0.0)
    for h in range(heads):
        sign = jnp.where((row >= rows) & (row % heads == h), -lambdas_ref[h], sign)
    position = iota((2 * rows, cache_len), 1)
    second = row % rows >= heads

    def query_of(s):
        even, odd = q_scr[s], q_scr[s + 1]
        return jnp.concatenate([even[:heads], odd[:heads], even[heads:], odd[heads:]], axis=0)

    def scores_of(step):
        found = []
        for b in range(0, block, 2):
            s = step * block + b
            even, odd = kv_ref[s], kv_ref[s + 1]
            query = query_of(s)
            keys = jnp.concatenate([even[:, :v_width], odd[:, :v_width]], axis=1)
            values = jnp.concatenate([odd[:, v_width:], even[:, v_width:]], axis=1)
            fresh = query * jnp.where(second, k_scr[s + 1 : s + 2], k_scr[s : s + 1])
            fresh = jnp.sum(fresh, axis=1, keepdims=True)
            found.append((dot_nt(query.astype(bf16), keys), fresh, values))
        return found

    def weights_of(step, found):
        made = []
        for b in range(0, block, 2):
            s = step * block + b
            scores, fresh, values = found[b // 2]
            length = jnp.where(second, lengths_ref[s + 1], lengths_ref[s])
            scores = jnp.where(position < length, scores * scaling, neg_fill)
            fresh = fresh * scaling
            top = jnp.maximum(jnp.max(scores, axis=1, keepdims=True), fresh)
            expo = jnp.exp(scores - top)
            expo_new = jnp.exp(fresh - top)
            factor = sign / (jnp.sum(expo, axis=1, keepdims=True) + expo_new)
            part = expo * factor
            part_new = expo_new * factor
            weights = (part[:rows] + part[rows:]).astype(bf16)
            weight_new = (part_new[:rows] + part_new[rows:]).astype(bf16).astype(f32)
            value_new = jnp.where(second[:rows], v_scr[s + 1 : s + 2], v_scr[s : s + 1])
            made.append((weights, weight_new * value_new, values))
        return made

    def mix_values(step, made):
        for b in range(0, block, 2):
            weights, newest, values = made[b // 2]
            o_scr[(step * block + b) // 2] = dot(weights, values) + newest

    found, made = None, None
    for step in range(steps + 2):
        if step < steps:
            streams[step].wait()
        if step >= 2:
            mix_values(step - 2, made)
        if 1 <= step <= steps:
            made = weights_of(step - 1, found)
        if step < steps:
            found = scores_of(step)

    gains = jnp.concatenate([head_gain_ref[...], head_gain_ref[...]], axis=1)
    half = upper[: seqs // 2]
    for i in range(2):
        outs = []
        for h in range(heads):
            mix = jnp.where(half == (i == 0), o_scr[:, i * heads + h, :], 0.0)
            mean = jnp.sum(mix * mix, axis=1, keepdims=True) * (1.0 / v_width)
            mix = mix * lax.rsqrt(mean + epsilon)
            turned = pltpu.roll(mix, v_width, 1)
            outs.append((turned, mix) if i == 0 else (mix, turned))
        for p in range(heads // 2):
            out = jnp.where(half, outs[2 * p + 1][1], outs[2 * p][0]) * gains
            q_scr[i :: 2, p, :] = out
    head_out = jnp.concatenate([q_scr[:, p, :] for p in range(heads // 2)], axis=1).astype(bf16)
    heads_ref[...] = head_out
    mix_scr[...] = dot(picks, head_out).astype(bf16)
    backs[1].start()
    for back in backs:
        back.wait()


def silu(values):
    return values / (1.0 + jnp.exp(-values))


def partner(index, d, count):
    return index ^ d if count & (count - 1) == 0 else (index + d) % count


def own_kernel(
    heads_ref,
    w_out_hbm,
    tokens_hbm,
    gain_hbm,
    ffn_ref,
    base_ref,
    gain_ref,
    kept_ref,
    tokens_ref,
    rest_ref,
    res_scr,
    sems,
):
    tp_count, seqs, width = heads_ref.shape
    share = base_ref.shape[1]
    blocks = column_blocks(w_out_hbm, rest_ref, (kept_ref,))
    copies = [
        pltpu.make_async_copy(source, target, sems.at[i])
        for i, (source, target) in enumerate(
            [(tokens_hbm, tokens_ref), (gain_hbm, gain_ref), *blocks]
        )
    ]
    for copy in copies:
        copy.start()
    for copy in copies[:2]:
        copy.wait()
    square = jnp.zeros((seqs, 1), f32)
    for n, (_, w_out_ref) in enumerate(blocks):
        copies[2 + n].wait()
        cut = slice(n * share, (n + 1) * share)
        total = tokens_ref[:, cut].astype(f32)
        parts = jnp.zeros_like(total)
        for j in range(tp_count):
            part = dot(heads_ref[j], w_out_ref[j * width : (j + 1) * width])
            parts = parts + part.astype(bf16).astype(f32)
        residual = (total + parts).astype(bf16).astype(f32)
        res_scr[:, cut] = residual
        square = square + jnp.sum(residual * residual, axis=1, keepdims=True)
    scale = lax.rsqrt(square * (1.0 / res_scr.shape[1]) + epsilon)
    start = pl.multiple_of(lax.axis_index("tp") * share, share)
    base_ref[...] = res_scr[:, pl.ds(start, share)]
    ffn_ref[...] = (res_scr[...] * scale * gain_ref[...]).astype(bf16)


def shared_kernel(
    capacity,
    experts,
    ffn_ref,
    residual_ref,
    _,
    gate_hbm,
    up_hbm,
    down_hbm,
    routing_hbm,
    rates_hbm,
    *refs,
):
    seqs, share = residual_ref.shape
    tp_count = ffn_ref.shape[1] // share
    part_refs = refs[: tp_count - 1]
    (
        base_ref,
        mix_ref,
        gate_ref,
        up_ref,
        down_ref,
        routing_ref,
        rates_ref,
        slot_scr,
        sems,
    ) = refs[tp_count - 1 :]
    copies = [
        pltpu.make_async_copy(source, target, sems.at[i])
        for i, (source, target) in enumerate(
            [
                (routing_hbm, routing_ref),
                (rates_hbm, rates_ref),
                (gate_hbm, gate_ref),
                (up_hbm, up_ref),
                (down_hbm, down_ref),
            ]
        )
    ]
    for copy in copies:
        copy.start()
    for copy in copies[:2]:
        copy.wait()
    slots = own_slots(routing_ref, slot_scr, seqs, experts, capacity)
    top_count = rates_ref.shape[0]
    rates = jnp.concatenate([rates_ref[...], jnp.zeros((8 - top_count, seqs), f32)], axis=0)
    rates = jnp.concatenate([rates, jnp.zeros((8, 128 - seqs), f32)], axis=1).T[:seqs]
    ids = iota((seqs, experts * capacity), 1)
    mixing = jnp.zeros((seqs, experts * capacity), f32)
    for k, slot in enumerate(slots):
        mixing = jnp.where(slot == ids, rates[:, k : k + 1], mixing)
    high = mixing.astype(bf16)
    mix_ref[:seqs] = high
    mix_ref[seqs:] = (mixing - high.astype(f32)).astype(bf16)
    for copy in copies[2:4]:
        copy.wait()
    ffn_in = ffn_ref[...]
    act = silu(dot(ffn_in, gate_ref[...])) * dot(ffn_in, up_ref[...])
    act = act.astype(bf16)
    copies[4].wait()
    for d in range(tp_count):
        start = pl.multiple_of(partner(lax.axis_index("tp"), d, tp_count) * share, share)
        part = dot(act, down_ref[:, pl.ds(start, share)])
        if d:
            part_refs[d - 1][...] = part.astype(bf16)
        else:
            base_ref[...] = residual_ref[...] + part


def column_blocks(w_out_hbm, rest_ref, kept_refs):
    share = rest_ref.shape[2]
    targets = [*kept_refs, *[rest_ref.at[i] for i in range(rest_ref.shape[0])]]
    return [
        (w_out_hbm.at[:, pl.ds(n * share, share)], target) for n, target in enumerate(targets)
    ]


def expert_kernel(
    direct,
    kept,
    arrived_ref,
    gain_ref,
    *refs,
):
    kept_refs = refs[:kept]
    (
        w_out_hbm,
        gate_hbm,
        up_hbm,
        down_hbm,
        send_hbm,
        send_ref,
        rest_ref,
        gate_ref,
        up_ref,
        down_ref,
        res_scr,
        sems,
    ) = refs[kept:]
    blocks = column_blocks(w_out_hbm, rest_ref, kept_refs)
    copies = [
        pltpu.make_async_copy(source, target, sems.at[i])
        for i, (source, target) in enumerate(
            [
                *blocks[kept:],
                (gate_hbm, gate_ref),
                (up_hbm, up_ref),
                *column_blocks(down_hbm, down_ref, ()),
            ]
        )
    ]
    for copy in copies:
        copy.start()
    groups, chunk, packed = arrived_ref.shape
    rows, model = res_scr.shape
    capacity = rows // groups
    tp_count = chunk // capacity
    share = model // tp_count
    width = packed - share
    lefts = []
    tokens = []
    for j in range(tp_count):
        piece = arrived_ref[:, j * capacity : (j + 1) * capacity, :].astype(f32)
        piece = piece.reshape(rows, packed)
        lefts.append(piece[:, :width].astype(bf16))
        tokens.append(piece[:, width:])
    square = jnp.zeros((rows, 1), f32)
    for n in range(tp_count):
        if n >= kept:
            copies[n - kept].wait()
        w_out_ref = blocks[n][1]
        cut = slice(n * share, (n + 1) * share)
        total = jnp.zeros((rows, share), f32)
        for j in range(tp_count):
            part = dot(lefts[j], w_out_ref[j * width : (j + 1) * width])
            total = total + part.astype(bf16).astype(f32)
        residual = (tokens[n] + total).astype(bf16).astype(f32)
        res_scr[:, cut] = residual
        square = square + jnp.sum(residual * residual, axis=1, keepdims=True)
    scale = lax.rsqrt(square * (1.0 / model) + epsilon)
    ffn_in = (res_scr[...] * scale * gain_ref[...]).astype(bf16)
    copies[tp_count - kept].wait()
    gate = dot(ffn_in, gate_ref[...])
    copies[tp_count - kept + 1].wait()
    act = (silu(gate) * dot(ffn_in, up_ref[...])).astype(bf16)
    for n in range(tp_count):
        copies[n - tp_count].wait()
        result = dot(act, down_ref[n])
        if direct:
            for i in range(groups):
                first = (i * tp_count + n) * capacity
                send_ref[first : first + capacity, :] = result[
                    i * capacity : (i + 1) * capacity
                ].astype(bf16)
        else:
            send_ref[:, n * share : (n + 1) * share] = result.astype(bf16)
    back = pltpu.make_async_copy(send_ref, send_hbm, sems.at[0])
    back.start()
    back.wait()


def combine_kernel(base_ref, mix_ref, returned_ref, *refs):
    *part_refs, out_ref = refs
    seqs = out_ref.shape[0]
    returned = returned_ref[...]
    routed = dot(mix_ref[...], returned)
    shared = base_ref[...]
    for part_ref in part_refs:
        shared = shared + part_ref[...].astype(f32)
    out_ref[...] = (shared + routed[:seqs] + routed[seqs:]).astype(bf16)


def params(mib, **more):
    return pltpu.CompilerParams(vmem_limit_bytes=mib << 20, **more)


def shards(
    tokens,
    kv_cache,
    lengths,
    attn_gain,
    w_query,
    w_key,
    w_value,
    lambdas,
    head_gain,
    w_out,
    ffn_gain,
    w_shared_gate,
    w_shared_up,
    w_shared_down,
    routing,
    route_weights,
    w_exp_gate,
    w_exp_up,
    w_exp_down,
):
    seqs, width = tokens.shape
    tp_count = lax.axis_size("tp")
    ep_count = lax.axis_size("ep")
    devices = ep_count * tp_count
    top_count = routing.shape[1]
    experts = w_exp_gate.shape[0] * devices
    capacity = max(2, 2 * seqs * top_count // experts)
    cache_len, lanes = kv_cache.shape[1:]
    v_width = head_gain.shape[0]
    heads = lambdas.shape[0]
    share = width // tp_count
    local = heads * v_width
    packed = local + share
    direct = capacity % 8 == 0
    block = 4
    head_out, send = pl.pallas_call(
        functools.partial(attention_kernel, capacity, experts, block),
        in_specs=[HBM] * 10,
        out_specs=[VMEM, HBM],
        out_shape=[
            pltpu.VMEM((seqs, local), bf16),
            jax.ShapeDtypeStruct((devices * capacity, packed), bf16),
        ],
        scratch_shapes=[
            pltpu.VMEM(tokens.shape, bf16),
            pltpu.VMEM((1, width), f32),
            pltpu.VMEM(w_query.shape, bf16),
            pltpu.VMEM(w_key.shape[::-1], bf16),
            pltpu.VMEM(w_value.shape[::-1], bf16),
            pltpu.VMEM((1, v_width), f32),
            pltpu.VMEM(routing.shape[::-1], jnp.int32),
            pltpu.SMEM(lengths.shape, jnp.int32),
            pltpu.SMEM(lambdas.shape, f32),
            pltpu.VMEM(kv_cache.shape, bf16),
            pltpu.VMEM((seqs, 2 * heads, lanes), f32),
            pltpu.VMEM((seqs, lanes), f32),
            pltpu.VMEM((seqs, lanes), f32),
            pltpu.VMEM((seqs // 2, 2 * heads, lanes), f32),
            pltpu.VMEM((routing.shape[0], 8), f32),
            pltpu.VMEM((devices * capacity, share), bf16),
            pltpu.VMEM((devices * capacity, local), bf16),
            pltpu.SemaphoreType.DMA((9,)),
            pltpu.SemaphoreType.DMA((seqs // block,)),
            pltpu.SemaphoreType.DMA((2,)),
        ],
        compiler_params=pltpu.CompilerParams(vmem_limit_bytes=67_043_328 - 2 * seqs * local),
        cost_estimate=pl.CostEstimate(
            flops=seqs * cache_len * lanes * 32, bytes_accessed=kv_cache.size * 2, transcendentals=0
        ),
        name="attention",
    )(
        tokens,
        attn_gain.reshape(1, width),
        w_query,
        w_key.T,
        w_value.T,
        head_gain.reshape(1, v_width),
        routing.T,
        lengths,
        lambdas,
        kv_cache,
    )

    arrived = lax.all_to_all(send, ("ep", "tp"), split_axis=0, concat_axis=0, tiled=True)
    arrived = arrived.reshape(ep_count, tp_count * capacity, packed)
    all_heads = lax.all_gather(head_out, "tp", axis=0, tiled=False)

    exp_gate = w_exp_gate.reshape(w_exp_gate.shape[1:])
    exp_up = w_exp_up.reshape(w_exp_up.shape[1:])
    exp_down = w_exp_down.reshape(w_exp_down.shape[1:])
    rows = ep_count * capacity
    w_out_block = (w_out.shape[0], share)
    rest = pltpu.VMEM((tp_count - 1, *w_out_block), bf16)
    ffn_own, residual, gain, kept = pl.pallas_call(
        own_kernel,
        in_specs=[VMEM] + [HBM] * 3,
        out_specs=[VMEM] * 4,
        out_shape=[
            pltpu.VMEM((seqs, width), bf16),
            pltpu.VMEM((seqs, share), f32),
            pltpu.VMEM((1, width), f32),
            pltpu.VMEM(w_out_block, bf16),
        ],
        scratch_shapes=[
            pltpu.VMEM(tokens.shape, bf16),
            rest,
            pltpu.VMEM((seqs, width), f32),
            pltpu.SemaphoreType.DMA((2 + tp_count,)),
        ],
        compiler_params=pltpu.CompilerParams(vmem_limit_bytes=63_900_000),
        cost_estimate=pl.CostEstimate(
            flops=2 * seqs * w_out.size, bytes_accessed=4 << 20, transcendentals=0
        ),
        name="own",
    )(all_heads, w_out, tokens, ffn_gain.reshape(1, width))
    arrived, gain, kept = [
        pltpu.with_memory_space_constraint(value, pltpu.VMEM) for value in (arrived, gain, kept)
    ]

    sent_shape = (devices * capacity, share) if direct else (rows, width)
    sent = pl.pallas_call(
        functools.partial(expert_kernel, direct, 1),
        in_specs=[VMEM] * 3 + [HBM] * 4,
        out_specs=HBM,
        out_shape=jax.ShapeDtypeStruct(sent_shape, bf16),
        scratch_shapes=[
            pltpu.VMEM(sent_shape, bf16),
            rest,
            pltpu.VMEM(exp_gate.shape, bf16),
            pltpu.VMEM(exp_up.shape, bf16),
            pltpu.VMEM((tp_count, exp_down.shape[0], share), bf16),
            pltpu.VMEM((rows, width), f32),
            pltpu.SemaphoreType.DMA((1 + 2 * tp_count,)),
        ],
        compiler_params=pltpu.CompilerParams(vmem_limit_bytes=60 * 1024 * 1024),
        cost_estimate=pl.CostEstimate(
            flops=2 * rows * 5 * w_out.size // 2, bytes_accessed=1 << 20, transcendentals=0
        ),
        name="experts",
    )(arrived, gain, kept, w_out, exp_gate, exp_up, exp_down)
    if not direct:
        sent = sent.reshape(ep_count, capacity, tp_count, share)
        sent = sent.transpose(0, 2, 1, 3).reshape(devices * capacity, share)
    returned = lax.all_to_all(sent, ("ep", "tp"), split_axis=0, concat_axis=0, tiled=True)
    *part, base, mix = pl.pallas_call(
        functools.partial(shared_kernel, capacity, experts),
        in_specs=[VMEM] * 2 + [HBM] * 6,
        out_specs=[VMEM] * (tp_count + 1),
        out_shape=[pltpu.VMEM((seqs, share), bf16)] * (tp_count - 1)
        + [
            pltpu.VMEM((seqs, share), f32),
            pltpu.VMEM((2 * seqs, experts * capacity), bf16),
        ],
        scratch_shapes=[
            pltpu.VMEM(w_shared_gate.shape, bf16),
            pltpu.VMEM(w_shared_up.shape, bf16),
            pltpu.VMEM(w_shared_down.shape, bf16),
            pltpu.VMEM(routing.shape[::-1], jnp.int32),
            pltpu.VMEM(route_weights.shape[::-1], f32),
            pltpu.VMEM((routing.shape[0], 8), f32),
            pltpu.SemaphoreType.DMA((5,)),
        ],
        compiler_params=pltpu.CompilerParams(vmem_limit_bytes=65_500_000),
        cost_estimate=pl.CostEstimate(
            flops=2 * seqs * 3 * w_shared_up.size, bytes_accessed=3 << 19, transcendentals=0
        ),
        name="shared",
    )(
        ffn_own,
        residual,
        sent,
        w_shared_gate,
        w_shared_up,
        w_shared_down,
        routing.T,
        route_weights.T,
    )
    parts = [
        lax.ppermute(piece, "tp", [(i, partner(i, d, tp_count)) for i in range(tp_count)])
        for d, piece in enumerate(part, 1)
    ]

    return pl.pallas_call(
        combine_kernel,
        in_specs=[VMEM] * (tp_count + 2),
        out_specs=VMEM,
        out_shape=jax.ShapeDtypeStruct((seqs, share), bf16),
        compiler_params=params(16),
        name="combine",
    )(base, mix, returned, *parts)


def solution(mesh):
    return jax.shard_map(
        shards,
        mesh=mesh,
        in_specs=(
            P("ep", None),
            P("ep", None, "tp"),
            P("ep"),
            P(),
            P(None, "tp"),
            P(None, "tp"),
            P(None, "tp"),
            P("tp"),
            P(),
            P(),
            P(),
            P(None, "tp"),
            P(None, "tp"),
            P("tp", None),
            P(),
            P("ep", None),
            P(("ep", "tp"), None, None),
            P(("ep", "tp"), None, None),
            P(("ep", "tp"), None, None),
        ),
        out_specs=P("ep", "tp"),
        check_vma=False,
    )
```

```python
import functools

import jax
import jax.numpy as jnp
from jax import lax
from jax.experimental import pallas as pl
from jax.experimental.pallas import tpu as pltpu
from jax.sharding import PartitionSpec as P


epsilon = 1e-06
neg_fill = -1e30
f32 = jnp.float32
bf16 = jnp.bfloat16
VMEM = pl.BlockSpec(memory_space=pltpu.VMEM)
SMEM = pl.BlockSpec(memory_space=pltpu.SMEM)
HBM = pl.BlockSpec(memory_space=pltpu.HBM)


def iota(shape, axis):
    return lax.broadcasted_iota(jnp.int32, shape, axis)


def dot(a, b):
    return jnp.dot(a, b, preferred_element_type=f32)


def dot_nt(a, b):
    return lax.dot_general(a, b, (((1,), (1,)), ((), ())), preferred_element_type=f32)


def inv_rms(values):
    return lax.rsqrt(jnp.mean(values * values, axis=-1, keepdims=True) + epsilon)


def slots_of(routing, experts, capacity, tp_count):
    rows, top_count = routing.shape
    ids = iota((rows, experts), 1).astype(f32)
    columns = [routing[:, k : k + 1] for k in range(top_count)]
    hits = [column == ids for column in columns]
    present = jnp.zeros((rows, experts), f32)
    for hit in hits:
        present = jnp.where(hit, 1.0, present)
    earlier = (iota((rows, rows), 1) < iota((rows, rows), 0)).astype(bf16)
    before = dot(earlier, present.astype(bf16))
    slots = []
    for column, hit in zip(columns, hits):
        rank = jnp.sum(jnp.where(hit, before, 0.0), axis=1, keepdims=True)
        across = jnp.floor((column + 0.5) * (1.0 / tp_count))
        device = (column - across * tp_count) * (experts // tp_count) + across
        slots.append((device * capacity + rank).astype(jnp.int32))
    return slots


def own_slots(routing_ref, slot_scr, seqs, experts, capacity, tp_count):
    top_count, batch = routing_ref.shape
    pad = jnp.zeros((8 - top_count, batch), f32)
    slot_scr[...] = jnp.concatenate([routing_ref[...].astype(f32), pad], axis=0).T
    start = pl.multiple_of(lax.axis_index("ep") * seqs, seqs)
    return slots_of(slot_scr[pl.ds(start, seqs), :top_count], experts, capacity, tp_count)


def attention_kernel(
    capacity,
    experts,
    tp_count,
    block,
    tokens_hbm,
    attn_gain_hbm,
    w_query_hbm,
    w_key_hbm,
    w_value_hbm,
    head_gain_hbm,
    routing_hbm,
    lengths_hbm,
    lambdas_hbm,
    kv_hbm,
    heads_ref,
    send_hbm,
    tokens_ref,
    attn_gain_ref,
    w_query_ref,
    w_key_ref,
    w_value_ref,
    head_gain_ref,
    routing_ref,
    lengths_ref,
    lambdas_ref,
    kv_ref,
    q_scr,
    k_scr,
    v_scr,
    o_scr,
    slot_scr,
    back_scr,
    mix_scr,
    sems,
    kv_sems,
    back_sems,
):
    seqs, rows, lanes = q_scr.shape
    heads = rows // 2
    v_width = lanes // 2
    qk_width = v_width // 2
    cache_len = kv_ref.shape[1]
    width = mix_scr.shape[1]
    share = back_scr.shape[1]
    scaling = qk_width ** (-0.5)
    copies = [
        pltpu.make_async_copy(source, target, sems.at[i])
        for i, (source, target) in enumerate(
            [
                (tokens_hbm, tokens_ref),
                (attn_gain_hbm, attn_gain_ref),
                (routing_hbm, routing_ref),
                (w_query_hbm, w_query_ref),
                (w_key_hbm, w_key_ref),
                (w_value_hbm, w_value_ref),
                (lengths_hbm, lengths_ref),
                (lambdas_hbm, lambdas_ref),
                (head_gain_hbm, head_gain_ref),
            ]
        )
    ]
    for copy in copies:
        copy.start()
    steps = seqs // block
    streams = [
        pltpu.make_async_copy(
            kv_hbm.at[pl.ds(i * block, block)], kv_ref.at[pl.ds(i * block, block)], kv_sems.at[i]
        )
        for i in range(steps)
    ]
    streams[0].start()
    for copy in copies[:3]:
        copy.wait()
    for stream in streams[1:]:
        stream.start()

    slots = own_slots(routing_ref, slot_scr, seqs, experts, capacity, tp_count)
    ids = iota((seqs, experts * capacity), 1)
    picks = jnp.zeros((seqs, experts * capacity), f32)
    for slot in slots:
        picks = jnp.where(slot == ids, 1.0, picks)
    picks = picks.T.astype(bf16)
    start = pl.multiple_of(lax.axis_index("tp") * share, share)
    back_scr[...] = dot(picks, tokens_ref[:, pl.ds(start, share)]).astype(bf16)
    backs = [
        pltpu.make_async_copy(back_scr, send_hbm.at[:, pl.ds(width, share)], back_sems.at[0]),
        pltpu.make_async_copy(mix_scr, send_hbm.at[:, pl.ds(0, width)], back_sems.at[1]),
    ]
    backs[0].start()
    tokens = tokens_ref[...].astype(f32)
    normed = (tokens * inv_rms(tokens) * attn_gain_ref[...]).astype(bf16)

    for copy in copies[3:]:
        copy.wait()
    queries = dot(normed, w_query_ref[...]).astype(bf16).astype(f32)
    key_new = dot_nt(normed, w_key_ref[...]).astype(bf16).astype(f32)
    value_new = dot_nt(normed, w_value_ref[...]).astype(bf16).astype(f32)
    k_scr[...] = jnp.concatenate([key_new, key_new], axis=1)
    v_scr[...] = jnp.concatenate([value_new, value_new], axis=1)
    lane = iota((seqs, lanes), 1)
    upper = lane >= v_width
    own_keys = upper == (iota((seqs, lanes), 0) % 2 == 1)
    for h in range(heads):
        pair = queries[:, (h // 2) * lanes : (h // 2 + 1) * lanes]
        pair = jnp.where(upper == (h % 2 == 1), pair, pltpu.roll(pair, v_width, 1))
        for m in range(2):
            inner = lane % v_width
            keep = own_keys & (inner >= m * qk_width) & (inner < (m + 1) * qk_width)
            q_scr[:, m * heads + h, :] = jnp.where(keep, pair, 0.0)

    row = iota((2 * rows, 1), 0)
    sign = jnp.where(row < rows, 1.0, 0.0)
    for h in range(heads):
        sign = jnp.where((row >= rows) & (row % heads == h), -lambdas_ref[h], sign)
    position = iota((2 * rows, cache_len), 1)
    second = row % rows >= heads

    def query_of(s):
        even, odd = q_scr[s], q_scr[s + 1]
        return jnp.concatenate([even[:heads], odd[:heads], even[heads:], odd[heads:]], axis=0)

    def scores_of(step):
        found = []
        for b in range(0, block, 2):
            s = step * block + b
            even, odd = kv_ref[s], kv_ref[s + 1]
            query = query_of(s)
            keys = jnp.concatenate([even[:, :v_width], odd[:, :v_width]], axis=1)
            values = jnp.concatenate([odd[:, v_width:], even[:, v_width:]], axis=1)
            fresh = query * jnp.where(second, k_scr[s + 1 : s + 2], k_scr[s : s + 1])
            fresh = jnp.sum(fresh, axis=1, keepdims=True)
            found.append((dot_nt(query.astype(bf16), keys), fresh, values))
        return found

    def weights_of(step, found):
        made = []
        for b in range(0, block, 2):
            s = step * block + b
            scores, fresh, values = found[b // 2]
            length = jnp.where(second, lengths_ref[s + 1], lengths_ref[s])
            scores = jnp.where(position < length, scores * scaling, neg_fill)
            fresh = fresh * scaling
            top = jnp.maximum(jnp.max(scores, axis=1, keepdims=True), fresh)
            expo = jnp.exp(scores - top)
            expo_new = jnp.exp(fresh - top)
            factor = sign / (jnp.sum(expo, axis=1, keepdims=True) + expo_new)
            part = expo * factor
            part_new = expo_new * factor
            weights = (part[:rows] + part[rows:]).astype(bf16)
            weight_new = (part_new[:rows] + part_new[rows:]).astype(bf16).astype(f32)
            value_new = jnp.where(second[:rows], v_scr[s + 1 : s + 2], v_scr[s : s + 1])
            made.append((weights, weight_new * value_new, values))
        return made

    def mix_values(step, made):
        for b in range(0, block, 2):
            weights, newest, values = made[b // 2]
            o_scr[(step * block + b) // 2] = dot(weights, values) + newest

    found, made = None, None
    for step in range(steps + 2):
        if step < steps:
            streams[step].wait()
        if step >= 2:
            mix_values(step - 2, made)
        if 1 <= step <= steps:
            made = weights_of(step - 1, found)
        if step < steps:
            found = scores_of(step)

    gains = jnp.concatenate([head_gain_ref[...], head_gain_ref[...]], axis=1)
    half = upper[: seqs // 2]
    for i in range(2):
        outs = []
        for h in range(heads):
            mix = jnp.where(half == (i == 0), o_scr[:, i * heads + h, :], 0.0)
            mean = jnp.sum(mix * mix, axis=1, keepdims=True) * (1.0 / v_width)
            mix = mix * lax.rsqrt(mean + epsilon)
            turned = pltpu.roll(mix, v_width, 1)
            outs.append((turned, mix) if i == 0 else (mix, turned))
        for p in range(heads // 2):
            out = jnp.where(half, outs[2 * p + 1][1], outs[2 * p][0]) * gains
            q_scr[i :: 2, p, :] = out
    head_out = jnp.concatenate([q_scr[:, p, :] for p in range(heads // 2)], axis=1).astype(bf16)
    heads_ref[...] = head_out
    mix_scr[...] = dot(picks, head_out).astype(bf16)
    backs[1].start()
    for back in backs:
        back.wait()


def silu(values):
    return values / (1.0 + jnp.exp(-values))


def partner(index, d, count):
    return index ^ d if count & (count - 1) == 0 else (index + d) % count


def own_kernel(
    heads_ref,
    w_out_hbm,
    tokens_hbm,
    gain_hbm,
    ffn_ref,
    base_ref,
    gain_ref,
    kept_ref,
    tokens_ref,
    rest_ref,
    res_scr,
    sems,
):
    tp_count, seqs, width = heads_ref.shape
    share = base_ref.shape[1]
    blocks = column_blocks(w_out_hbm, rest_ref, (kept_ref,))
    copies = [
        pltpu.make_async_copy(source, target, sems.at[i])
        for i, (source, target) in enumerate(
            [(tokens_hbm, tokens_ref), (gain_hbm, gain_ref), *blocks]
        )
    ]
    for copy in copies:
        copy.start()
    for copy in copies[:2]:
        copy.wait()
    square = jnp.zeros((seqs, 1), f32)
    for n, (_, w_out_ref) in enumerate(blocks):
        copies[2 + n].wait()
        cut = slice(n * share, (n + 1) * share)
        total = tokens_ref[:, cut].astype(f32)
        parts = jnp.zeros_like(total)
        for j in range(tp_count):
            part = dot(heads_ref[j], w_out_ref[j * width : (j + 1) * width])
            parts = parts + part.astype(bf16).astype(f32)
        residual = (total + parts).astype(bf16).astype(f32)
        res_scr[:, cut] = residual
        square = square + jnp.sum(residual * residual, axis=1, keepdims=True)
    scale = lax.rsqrt(square * (1.0 / res_scr.shape[1]) + epsilon)
    start = pl.multiple_of(lax.axis_index("tp") * share, share)
    base_ref[...] = res_scr[:, pl.ds(start, share)]
    ffn_ref[...] = (res_scr[...] * scale * gain_ref[...]).astype(bf16)


def shared_kernel(
    capacity,
    experts,
    ffn_ref,
    residual_ref,
    _,
    gate_hbm,
    up_hbm,
    down_hbm,
    routing_hbm,
    rates_hbm,
    *refs,
):
    seqs, share = residual_ref.shape
    tp_count = ffn_ref.shape[1] // share
    part_refs = refs[: tp_count - 1]
    (
        base_ref,
        mix_ref,
        gate_ref,
        up_ref,
        down_ref,
        routing_ref,
        rates_ref,
        slot_scr,
        sems,
    ) = refs[tp_count - 1 :]
    copies = [
        pltpu.make_async_copy(source, target, sems.at[i])
        for i, (source, target) in enumerate(
            [
                (routing_hbm, routing_ref),
                (rates_hbm, rates_ref),
                (gate_hbm, gate_ref),
                (up_hbm, up_ref),
                (down_hbm, down_ref),
            ]
        )
    ]
    for copy in copies:
        copy.start()
    for copy in copies[:2]:
        copy.wait()
    slots = own_slots(routing_ref, slot_scr, seqs, experts, capacity, tp_count)
    top_count = rates_ref.shape[0]
    rates = jnp.concatenate([rates_ref[...], jnp.zeros((8 - top_count, seqs), f32)], axis=0)
    rates = jnp.concatenate([rates, jnp.zeros((8, 128 - seqs), f32)], axis=1).T[:seqs]
    ids = iota((seqs, experts * capacity), 1)
    mixing = jnp.zeros((seqs, experts * capacity), f32)
    for k, slot in enumerate(slots):
        mixing = jnp.where(slot == ids, rates[:, k : k + 1], mixing)
    high = mixing.astype(bf16)
    mix_ref[:seqs] = high
    mix_ref[seqs:] = (mixing - high.astype(f32)).astype(bf16)
    for copy in copies[2:4]:
        copy.wait()
    ffn_in = ffn_ref[...]
    act = silu(dot(ffn_in, gate_ref[...])) * dot(ffn_in, up_ref[...])
    act = act.astype(bf16)
    copies[4].wait()
    for d in range(tp_count):
        start = pl.multiple_of(partner(lax.axis_index("tp"), d, tp_count) * share, share)
        part = dot(act, down_ref[:, pl.ds(start, share)])
        if d:
            part_refs[d - 1][...] = part.astype(bf16)
        else:
            base_ref[...] = residual_ref[...] + part


def column_blocks(w_out_hbm, rest_ref, kept_refs):
    share = rest_ref.shape[2]
    targets = [*kept_refs, *[rest_ref.at[i] for i in range(rest_ref.shape[0])]]
    return [
        (w_out_hbm.at[:, pl.ds(n * share, share)], target) for n, target in enumerate(targets)
    ]


def expert_kernel(
    kept,
    arrived_ref,
    gain_ref,
    *refs,
):
    kept_refs = refs[:kept]
    (
        w_out_hbm,
        gate_hbm,
        up_hbm,
        down_hbm,
        send_hbm,
        send_ref,
        rest_ref,
        gate_ref,
        up_ref,
        down_ref,
        res_scr,
        sems,
        back_sems,
    ) = refs[kept:]
    blocks = column_blocks(w_out_hbm, rest_ref, kept_refs)
    copies = [
        pltpu.make_async_copy(source, target, sems.at[i])
        for i, (source, target) in enumerate(
            [
                *blocks[kept:],
                (gate_hbm, gate_ref),
                (up_hbm, up_ref),
                *column_blocks(down_hbm, down_ref, ()),
            ]
        )
    ]
    for copy in copies:
        copy.start()
    tp_count, rows, packed = arrived_ref.shape
    model = res_scr.shape[1]
    share = model // tp_count
    width = packed - share
    lefts = []
    tokens = []
    for j in range(tp_count):
        lefts.append(arrived_ref[j, :, :width])
        tokens.append(arrived_ref[j, :, width:].astype(f32))
    square = jnp.zeros((rows, 1), f32)
    for n in range(tp_count):
        if n >= kept:
            copies[n - kept].wait()
        w_out_ref = blocks[n][1]
        cut = slice(n * share, (n + 1) * share)
        total = jnp.zeros((rows, share), f32)
        for j in range(tp_count):
            part = dot(lefts[j], w_out_ref[j * width : (j + 1) * width])
            total = total + part.astype(bf16).astype(f32)
        residual = (tokens[n] + total).astype(bf16).astype(f32)
        res_scr[:, cut] = residual
        square = square + jnp.sum(residual * residual, axis=1, keepdims=True)
    scale = lax.rsqrt(square * (1.0 / model) + epsilon)
    ffn_in = (res_scr[...] * scale * gain_ref[...]).astype(bf16)
    copies[tp_count - kept].wait()
    gate = dot(ffn_in, gate_ref[...])
    copies[tp_count - kept + 1].wait()
    act = (silu(gate) * dot(ffn_in, up_ref[...])).astype(bf16)
    backs = []
    for n in range(tp_count):
        copies[n - tp_count].wait()
        cut = pl.ds(n * rows, rows)
        send_ref[cut] = dot(act, down_ref[n]).astype(bf16)
        backs.append(pltpu.make_async_copy(send_ref.at[cut], send_hbm.at[cut], back_sems.at[n]))
        backs[n].start()
    for back in backs:
        back.wait()


def combine_kernel(base_ref, mix_ref, returned_ref, *refs):
    *part_refs, out_ref = refs
    seqs = out_ref.shape[0]
    returned = returned_ref[...]
    routed = dot(mix_ref[...], returned)
    shared = base_ref[...]
    for part_ref in part_refs:
        shared = shared + part_ref[...].astype(f32)
    out_ref[...] = (shared + routed[:seqs] + routed[seqs:]).astype(bf16)


def params(mib, **more):
    return pltpu.CompilerParams(vmem_limit_bytes=mib << 20, **more)


def shards(
    tokens,
    kv_cache,
    lengths,
    attn_gain,
    w_query,
    w_key,
    w_value,
    lambdas,
    head_gain,
    w_out,
    ffn_gain,
    w_shared_gate,
    w_shared_up,
    w_shared_down,
    routing,
    route_weights,
    w_exp_gate,
    w_exp_up,
    w_exp_down,
):
    seqs, width = tokens.shape
    tp_count = lax.axis_size("tp")
    ep_count = lax.axis_size("ep")
    devices = ep_count * tp_count
    top_count = routing.shape[1]
    experts = w_exp_gate.shape[0] * devices
    capacity = max(2, 2 * seqs * top_count // experts)
    cache_len, lanes = kv_cache.shape[1:]
    v_width = head_gain.shape[0]
    heads = lambdas.shape[0]
    share = width // tp_count
    local = heads * v_width
    packed = local + share
    block = 8
    head_out, send = pl.pallas_call(
        functools.partial(attention_kernel, capacity, experts, tp_count, block),
        in_specs=[HBM] * 10,
        out_specs=[VMEM, HBM],
        out_shape=[
            pltpu.VMEM((seqs, local), bf16),
            jax.ShapeDtypeStruct((devices * capacity, packed), bf16),
        ],
        scratch_shapes=[
            pltpu.VMEM(tokens.shape, bf16),
            pltpu.VMEM((1, width), f32),
            pltpu.VMEM(w_query.shape, bf16),
            pltpu.VMEM(w_key.shape[::-1], bf16),
            pltpu.VMEM(w_value.shape[::-1], bf16),
            pltpu.VMEM((1, v_width), f32),
            pltpu.VMEM(routing.shape[::-1], jnp.int32),
            pltpu.SMEM(lengths.shape, jnp.int32),
            pltpu.SMEM(lambdas.shape, f32),
            pltpu.VMEM(kv_cache.shape, bf16),
            pltpu.VMEM((seqs, 2 * heads, lanes), f32),
            pltpu.VMEM((seqs, lanes), f32),
            pltpu.VMEM((seqs, lanes), f32),
            pltpu.VMEM((seqs // 2, 2 * heads, lanes), f32),
            pltpu.VMEM((routing.shape[0], 8), f32),
            pltpu.VMEM((devices * capacity, share), bf16),
            pltpu.VMEM((devices * capacity, local), bf16),
            pltpu.SemaphoreType.DMA((9,)),
            pltpu.SemaphoreType.DMA((seqs // block,)),
            pltpu.SemaphoreType.DMA((2,)),
        ],
        compiler_params=pltpu.CompilerParams(vmem_limit_bytes=67_043_328 - 2 * seqs * local),
        cost_estimate=pl.CostEstimate(
            flops=seqs * cache_len * lanes * 32, bytes_accessed=kv_cache.size * 2, transcendentals=0
        ),
        name="attention",
    )(
        tokens,
        attn_gain.reshape(1, width),
        w_query,
        w_key.T,
        w_value.T,
        head_gain.reshape(1, v_width),
        routing.T,
        lengths,
        lambdas,
        kv_cache,
    )

    arrived = lax.all_to_all(send, ("tp", "ep"), split_axis=0, concat_axis=0, tiled=True)
    arrived = arrived.reshape(tp_count, ep_count * capacity, packed)
    all_heads = lax.all_gather(head_out, "tp", axis=0, tiled=False)

    exp_gate = w_exp_gate.reshape(w_exp_gate.shape[1:])
    exp_up = w_exp_up.reshape(w_exp_up.shape[1:])
    exp_down = w_exp_down.reshape(w_exp_down.shape[1:])
    rows = ep_count * capacity
    w_out_block = (w_out.shape[0], share)
    rest = pltpu.VMEM((tp_count - 1, *w_out_block), bf16)
    ffn_own, residual, gain, kept = pl.pallas_call(
        own_kernel,
        in_specs=[VMEM] + [HBM] * 3,
        out_specs=[VMEM] * 4,
        out_shape=[
            pltpu.VMEM((seqs, width), bf16),
            pltpu.VMEM((seqs, share), f32),
            pltpu.VMEM((1, width), f32),
            pltpu.VMEM(w_out_block, bf16),
        ],
        scratch_shapes=[
            pltpu.VMEM(tokens.shape, bf16),
            rest,
            pltpu.VMEM((seqs, width), f32),
            pltpu.SemaphoreType.DMA((2 + tp_count,)),
        ],
        compiler_params=pltpu.CompilerParams(vmem_limit_bytes=63_900_000),
        cost_estimate=pl.CostEstimate(
            flops=2 * seqs * w_out.size, bytes_accessed=4 << 20, transcendentals=0
        ),
        name="own",
    )(all_heads, w_out, tokens, ffn_gain.reshape(1, width))
    arrived, gain, kept = [
        pltpu.with_memory_space_constraint(value, pltpu.VMEM) for value in (arrived, gain, kept)
    ]

    sent_shape = (devices * capacity, share)
    sent = pl.pallas_call(
        functools.partial(expert_kernel, 1),
        in_specs=[VMEM] * 3 + [HBM] * 4,
        out_specs=HBM,
        out_shape=jax.ShapeDtypeStruct(sent_shape, bf16),
        scratch_shapes=[
            pltpu.VMEM(sent_shape, bf16),
            rest,
            pltpu.VMEM(exp_gate.shape, bf16),
            pltpu.VMEM(exp_up.shape, bf16),
            pltpu.VMEM((tp_count, exp_down.shape[0], share), bf16),
            pltpu.VMEM((rows, width), f32),
            pltpu.SemaphoreType.DMA((1 + 2 * tp_count,)),
            pltpu.SemaphoreType.DMA((tp_count,)),
        ],
        compiler_params=pltpu.CompilerParams(vmem_limit_bytes=60 * 1024 * 1024),
        cost_estimate=pl.CostEstimate(
            flops=2 * rows * 5 * w_out.size // 2, bytes_accessed=1 << 20, transcendentals=0
        ),
        name="experts",
    )(arrived, gain, kept, w_out, exp_gate, exp_up, exp_down)
    returned = lax.all_to_all(sent, ("tp", "ep"), split_axis=0, concat_axis=0, tiled=True)
    *part, base, mix = pl.pallas_call(
        functools.partial(shared_kernel, capacity, experts),
        in_specs=[VMEM] * 2 + [HBM] * 6,
        out_specs=[VMEM] * (tp_count + 1),
        out_shape=[pltpu.VMEM((seqs, share), bf16)] * (tp_count - 1)
        + [
            pltpu.VMEM((seqs, share), f32),
            pltpu.VMEM((2 * seqs, experts * capacity), bf16),
        ],
        scratch_shapes=[
            pltpu.VMEM(w_shared_gate.shape, bf16),
            pltpu.VMEM(w_shared_up.shape, bf16),
            pltpu.VMEM(w_shared_down.shape, bf16),
            pltpu.VMEM(routing.shape[::-1], jnp.int32),
            pltpu.VMEM(route_weights.shape[::-1], f32),
            pltpu.VMEM((routing.shape[0], 8), f32),
            pltpu.SemaphoreType.DMA((5,)),
        ],
        compiler_params=pltpu.CompilerParams(vmem_limit_bytes=65_500_000),
        cost_estimate=pl.CostEstimate(
            flops=2 * seqs * 3 * w_shared_up.size, bytes_accessed=3 << 19, transcendentals=0
        ),
        name="shared",
    )(
        ffn_own,
        residual,
        sent,
        w_shared_gate,
        w_shared_up,
        w_shared_down,
        routing.T,
        route_weights.T,
    )
    parts = [
        lax.ppermute(piece, "tp", [(i, partner(i, d, tp_count)) for i in range(tp_count)])
        for d, piece in enumerate(part, 1)
    ]

    return pl.pallas_call(
        combine_kernel,
        in_specs=[VMEM] * (tp_count + 2),
        out_specs=VMEM,
        out_shape=jax.ShapeDtypeStruct((seqs, share), bf16),
        compiler_params=params(16),
        name="combine",
    )(base, mix, returned, *parts)


def solution(mesh):
    return jax.shard_map(
        shards,
        mesh=mesh,
        in_specs=(
            P("ep", None),
            P("ep", None, "tp"),
            P("ep"),
            P(),
            P(None, "tp"),
            P(None, "tp"),
            P(None, "tp"),
            P("tp"),
            P(),
            P(),
            P(),
            P(None, "tp"),
            P(None, "tp"),
            P("tp", None),
            P(),
            P("ep", None),
            P(("ep", "tp"), None, None),
            P(("ep", "tp"), None, None),
            P(("ep", "tp"), None, None),
        ),
        out_specs=P("ep", "tp"),
        check_vma=False,
    )
```
